128 devices in a mesh: sp: 32 (over z, y, core), tp: 4 (over x).
Axes of the slice: x: 4, y: 4, z: 4, core: 2. Of those that a mesh axis runs over, the one named last changes fastest.
Arguments:
- residual_in: bfloat16 [65536, 2048], P(('sp', 'tp')), may hold values from -6 to 6
- conv_input: bfloat16 [65536, 1024], P('sp', 'tp'), may hold values from -6 to 6
- input_gate: bfloat16 [65536, 1024], P('sp', 'tp'), may hold values from -6 to 6
- output_gate: bfloat16 [65536, 1024], P('sp', 'tp'), may hold values from -6 to 6
- conv_taps: bfloat16 [3, 1024], P(None, 'tp'), may hold values from -3.5 to 3.5
- doc_ids: int32 [65536], P('sp'), may hold values from 0 to 15, never falling along the last dimension, each value on 1 to 8192 neighbouring positions
- proj_weight: bfloat16 [1024, 2048], replicated, may hold values from -0.1875 to 0.1875
- norm_gain: float32 [2048], replicated, may hold values from 0.1 to 1.9
- expert_ids: int32 [65536, 2], P(('sp', 'tp')), may hold values from 0 to 31, all different within a row; in each aligned block of 512 rows (0 to 511, 512 to 1023, ...) at most 64 rows name the same one
- expert_weight: float32 [65536, 2], P(('sp', 'tp')), may hold values from 0.05 to 1
- w_gate: bfloat16 [32, 2048, 512], P('sp'), may hold values from -0.125 to 0.125
- w_up: bfloat16 [32, 2048, 512], P('sp'), may hold values from -0.125 to 0.125
- w_down: bfloat16 [32, 512, 2048], P('sp'), may hold values from -0.25 to 0.25
Outputs:
- layer_out: bfloat16 [65536, 2048], P(('sp', 'tp'))
The draws below stay inside these ranges and needn't reach their ends.
Inputs may be any that keep to these rules, and one draw needn't show every extreme that they name: `doc_ids`: numbers never fall along the sequence; one document spans at most 8192 positions. `expert_ids`: a token's two experts differ; in each aligned block of rows that one device holds, no expert is named more than 64 times, a bound that some block reaches.
All inputs are finite; a program needn't handle non-finite values.
Results may differ from the reference program's by a relative error of at most 0.0047.
Values may be sent and summed in bfloat16 or wider, within the bound.
A program may use at most 128 MiB of HBM per device.

```python
import math
import jax
import jax.numpy as jnp
import numpy as np
from jax import lax

D = 2048
CONV = 1024
FFE = 512
EXPERTS = 32
KW = 3
CAP = 64
TOK_DEV = 2048
TOKENS = 65536
SEG_COUNT = 16
DOC_MOST = 8192
N_SP = 32
N_TP = 4


def block_scale(rng, dims, cuts, smallest, high):
    def one(dim, parts):
        heights = jax.random.uniform(jax.random.fold_in(jax.random.fold_in(rng, 6), dim), (parts,), jnp.float32, smallest / len(cuts), high / len(cuts))
        return jnp.repeat(jnp.exp(heights), dims[dim] // parts).reshape((-1,) + (1,) * (len(dims) - dim - 1))

    loudness = one(*cuts[0])
    for cut in cuts[1:]:
        loudness = loudness * one(*cut)
    return loudness


def profile(amount, total, limit, skew):
    loads = [(1 << 20) // math.isqrt(grade ** skew) + 1 for grade in range(2, amount + 1)]
    surplus, holding = total - limit - (amount - 1), [1] * (amount - 1)
    while surplus > 0:
        free = [i for i in range(amount - 1) if holding[i] < limit]
        mass, budget = sum([loads[i] for i in free]), surplus
        for i in free:
            more = min(limit - holding[i], max(1, budget * loads[i] // mass), surplus)
            holding[i] = holding[i] + more
            surplus = surplus - more
    return np.array([limit] + holding)


def ragged_sizes(stream_key, number_of, total, reach, skew):
    if number_of == 2:
        one = jax.random.randint(stream_key, (), max(1, total - reach), min(reach, total - 1) + 1)
        return jnp.stack([one, total - one])
    sizes = jnp.asarray(profile(number_of, total, reach, skew), jnp.int32)
    couples = (number_of - 1) // 2
    giver, receiver = sizes[1:1 + 2 * couples:2], sizes[2:2 + 2 * couples:2]
    room = jnp.minimum(giver - 1, reach - receiver)
    moved = jax.random.randint(jax.random.fold_in(stream_key, 1), (couples,), 0, 1 << 20) % (room + 1)
    sizes = sizes.at[1:1 + 2 * couples:2].set(giver - moved).at[2:2 + 2 * couples:2].set(receiver + moved)
    return sizes[jax.random.permutation(jax.random.fold_in(stream_key, 2), number_of)]


def assign_block(rng, own, number, rows, number_of, top, bound, lean):
    ranking = jax.random.permutation(rng, number_of)
    packed, common = shares(number_of, rows * top, bound, lean, True), shares(number_of, rows * top, bound, lean, False)
    places = jnp.arange(number_of)

    def named(sizes, turn):
        used = int((sizes > 0).sum())
        fixed = max(1, used // 4)
        passed = fixed + (places - fixed + turn * (used - fixed)) % max(1, number_of - fixed)
        return jnp.zeros((number_of,), jnp.int32).at[ranking[jnp.where(places < fixed, places, passed)]].set(jnp.asarray(sizes, jnp.int32))

    sizes = jnp.where(number % 4 == 0, named(packed, number // 4), named(common, number - number // 4 - 1))
    mixed = jax.random.permutation(jax.random.fold_in(own, 3), number_of)
    donor, taker = mixed[0:number_of // 2 * 2:2], mixed[1:number_of // 2 * 2:2]
    slack = jnp.minimum(sizes[donor] - 1, bound - sizes[taker]) // 2
    slack = jnp.where((donor == ranking[0]) | (taker == ranking[0]) | (sizes[taker] == 0), 0, jnp.maximum(slack, 0))
    passed = jax.random.randint(jax.random.fold_in(own, 4), (number_of // 2,), 0, 1 << 20) % (slack + 1)
    sizes = sizes.at[donor].add(-passed).at[taker].add(passed)
    labels = jnp.searchsorted(jnp.cumsum(sizes), jnp.arange(rows * top), side="right").astype(jnp.int32)
    listing = labels.reshape(top, rows).T
    listing = listing[jax.random.permutation(jax.random.fold_in(own, 1), rows)]
    turn = jax.random.randint(jax.random.fold_in(own, 2), (rows, 1), 0, top)
    return jnp.take_along_axis(listing, (jnp.arange(top)[None, :] + turn) % top, axis=1)


def shares(amount, total, most, skew, full):
    weights = [(1 << 20) // math.isqrt(standing ** skew) + 1 for standing in range(1, amount + 1)]
    largest = most if full else min(most, max(-(-total // amount), total * weights[0] // sum(weights)))
    least = 1 if total - largest >= amount - 1 else 0
    counts, spare = [largest] + [least] * (amount - 1), total - largest - least * (amount - 1)
    while spare > 0:
        movable = [i for i in range(1, amount) if counts[i] < largest] or [i for i in range(1, amount) if counts[i] < most]
        mass, budget = sum([weights[i] for i in movable]), spare
        for i in movable:
            addition = min(most - counts[i], max(1, budget * weights[i] // mass), spare)
            counts[i] = counts[i] + addition
            spare = spare - addition
    return np.array(counts)


def centred(rng, extent, width, most, split=(), kind=jnp.bfloat16):
    values = width * jax.random.normal(rng, extent, jnp.float32)
    if split:
        values = values * block_scale(rng, extent, split, -0.22, 0.18)
    return jnp.clip(values, -most, most).astype(kind)


def setup_inputs(seed: int = 0) -> dict:
    key_of = jax.random.split(jax.random.key(seed), 14)
    residual_in = centred(key_of[0], (TOKENS, D), 1.0, 6.0, ((0, 128),))
    conv_input = centred(key_of[1], (TOKENS, CONV), 1.0, 6.0, ((0, 32), (1, 4)))
    input_gate = centred(key_of[2], (TOKENS, CONV), 1.0, 6.0, ((0, 32), (1, 4)))
    output_gate = centred(key_of[3], (TOKENS, CONV), 1.0, 6.0, ((0, 32), (1, 4)))
    conv_taps = centred(key_of[4], (KW, CONV), KW ** -0.5, 3.5, ((1, 4),))
    doc_ids = jnp.searchsorted(jnp.cumsum(ragged_sizes(key_of[5], SEG_COUNT, TOKENS, DOC_MOST, 2)), jnp.arange(TOKENS), side="right").astype(jnp.int32)
    proj_weight = centred(key_of[6], (CONV, D), CONV ** -0.5, 0.1875)
    norm_gain = jnp.clip(1.0 + 0.18 * jax.random.normal(key_of[7], (D,), jnp.float32), 0.1, 1.9)
    expert_ids_keys = jax.random.split(jax.random.fold_in(key_of[8], 1), TOKENS // (TOK_DEV // N_TP))
    expert_ids_turns = jax.random.permutation(jax.random.fold_in(key_of[8], 3), TOKENS // (TOK_DEV // N_TP))
    expert_ids = jax.vmap(lambda own, number: assign_block(jax.random.fold_in(key_of[8], 2), own, number, TOK_DEV // N_TP, EXPERTS, 2, CAP, 2))(expert_ids_keys, expert_ids_turns).reshape((TOKENS, 2))
    expert_weight = jnp.clip(jnp.exp(math.log(1.0) - 2.9957323 * jax.random.uniform(key_of[9], (TOKENS, 2), jnp.float32) ** block_scale(key_of[9], (TOKENS, 2), ((0, 128),), -0.2, 0.2)), 0.05, 1.0)
    w_gate = centred(key_of[10], (EXPERTS, D, FFE), D ** -0.5, 0.125, ((0, 32),))
    w_up = centred(key_of[11], (EXPERTS, D, FFE), D ** -0.5, 0.125, ((0, 32),))
    w_down = centred(key_of[12], (EXPERTS, FFE, D), FFE ** -0.5, 0.25, ((0, 32),))
    return dict(residual_in=residual_in, conv_input=conv_input, input_gate=input_gate, output_gate=output_gate, conv_taps=conv_taps, doc_ids=doc_ids, proj_weight=proj_weight, norm_gain=norm_gain, expert_ids=expert_ids, expert_weight=expert_weight, w_gate=w_gate, w_up=w_up, w_down=w_down)


epsilon = 1e-06

def reference(residual_in, conv_input, input_gate, output_gate, conv_taps, doc_ids, proj_weight, norm_gain, expert_ids, expert_weight, w_gate, w_up, w_down):
    product = input_gate.astype(jnp.float32) * conv_input.astype(jnp.float32)
    padded_in = jnp.concatenate([jnp.zeros((KW - 1, CONV), jnp.float32), product], axis=0)
    padded_ids = jnp.concatenate([jnp.full((KW - 1,), -1, jnp.int32), doc_ids.astype(jnp.int32)], axis=0)
    conv_sum = jnp.zeros((TOKENS, CONV), jnp.float32)
    for offset in range(KW):
        same_doc = padded_ids[offset:offset + TOKENS] == doc_ids
        term = conv_taps[offset].astype(jnp.float32)[None, :] * padded_in[offset:offset + TOKENS]
        conv_sum = conv_sum + jnp.where(same_doc[:, None], term, 0.0)
    gated = (output_gate.astype(jnp.float32) * conv_sum).astype(jnp.bfloat16)
    hidden = residual_in.astype(jnp.float32) + jnp.dot(gated, proj_weight, preferred_element_type=jnp.float32)
    scale_rows = lax.rsqrt(lax.optimization_barrier(jnp.mean(hidden * hidden, axis=-1, keepdims=True)) + epsilon)
    normed = (hidden * scale_rows * norm_gain[None, :]).astype(jnp.bfloat16)
    blocks = N_SP * N_TP
    block_rows = TOK_DEV // N_TP
    slots_all = blocks * CAP
    flat_ids = expert_ids.reshape(blocks, 2 * block_rows)
    one_hot = (flat_ids[:, :, None] == jnp.arange(EXPERTS, dtype=jnp.int32)[None, None, :]).astype(jnp.int32)
    before = jnp.cumsum(one_hot, axis=1) - one_hot
    slot_num = lax.optimization_barrier(jnp.sum(before * one_hot, axis=-1))
    slot_index = (jnp.arange(blocks, dtype=jnp.int32)[:, None] * CAP + slot_num).reshape(TOKENS, 2).astype(jnp.int32)

    def per_expert(total, expert):
        chosen = expert_ids == expert
        target = jnp.where(chosen, slot_index, slots_all)
        buffer = jnp.zeros((slots_all, D), jnp.bfloat16)
        buffer = buffer.at[target[:, 0]].set(normed, mode='drop')
        buffer = buffer.at[target[:, 1]].set(normed, mode='drop')
        gate_val = jnp.dot(buffer, w_gate[expert], preferred_element_type=jnp.float32)
        up_val = jnp.dot(buffer, w_up[expert], preferred_element_type=jnp.float32)
        act_rows = (jax.nn.silu(gate_val) * up_val).astype(jnp.bfloat16)
        out_rows = jnp.dot(act_rows, w_down[expert], preferred_element_type=jnp.float32).astype(jnp.bfloat16)
        for route in range(2):
            picked = out_rows[slot_index[:, route]].astype(jnp.float32) * expert_weight[:, route:route + 1]
            total = total + jnp.where(chosen[:, route:route + 1], picked, 0.0)
        return (total, None)
    expert_sum, unused = lax.scan(per_expert, jnp.zeros((TOKENS, D), jnp.float32), jnp.arange(EXPERTS, dtype=jnp.int32))
    return (hidden + expert_sum).astype(jnp.bfloat16)
```

```python
import jax
import jax.numpy as jnp
from jax import lax
from jax.sharding import PartitionSpec as P

EXPERTS = 32
CAP = 64
epsilon = 1e-06
F32 = jnp.float32
BF16 = jnp.bfloat16


def from_behind(x, axis, by):
    devices = lax.axis_size(axis)
    pairs = [(i, i + by) for i in range(devices) if 0 <= i + by < devices]
    return lax.ppermute(x, axis, pairs)


def per_device(
    residual_in,
    conv_input,
    input_gate,
    output_gate,
    conv_taps,
    doc_ids,
    proj_weight,
    norm_gain,
    expert_ids,
    expert_weight,
    w_gate,
    w_up,
    w_down,
):
    kernel_width = conv_taps.shape[0]
    rim = kernel_width - 1
    length, channels = conv_input.shape
    doc_float = doc_ids.astype(F32)
    tail = input_gate[-rim:].astype(F32) * conv_input[-rim:].astype(F32)
    packed = jnp.concatenate([tail, jnp.broadcast_to(doc_float[-rim:, None], (rim, 128))], axis=1)
    prev = from_behind(packed, "sp", 1)
    prev_in, prev_ids = prev[:, :channels], prev[:, channels]
    first = lax.axis_index("sp") == 0
    prev_ids = jnp.where(first, -1.0, prev_ids)
    product = input_gate.astype(F32) * conv_input.astype(F32)
    padded_in = jnp.concatenate([prev_in, product], axis=0)
    padded_ids = jnp.concatenate([prev_ids, doc_float], axis=0)
    conv_sum = jnp.zeros(product.shape, F32)
    for offset in range(kernel_width):
        same_doc = padded_ids[offset : offset + length] == doc_float
        term = conv_taps[offset].astype(F32)[None, :] * padded_in[offset : offset + length]
        conv_sum = conv_sum + jnp.where(same_doc[:, None], term, 0.0)
    gated = (output_gate.astype(F32) * conv_sum).astype(BF16)
    regrouped = lax.all_to_all(gated, "tp", split_axis=0, concat_axis=1, tiled=True)

    tokens = expert_ids.shape[0]
    experts = jnp.arange(EXPERTS, dtype=jnp.int32)
    ids_t = expert_ids.T
    weight_t = expert_weight.T
    hit = [ids_t[j][None, :] == experts[:, None] for j in range(2)]
    used = hit[0] | hit[1]
    weight_of = jnp.where(hit[0], weight_t[0][None, :], 0.0) + jnp.where(hit[1], weight_t[1][None, :], 0.0)
    t_row = lax.broadcasted_iota(jnp.int32, (tokens, tokens), 0)
    t_col = lax.broadcasted_iota(jnp.int32, (tokens, tokens), 1)
    earlier = (t_row < t_col).astype(BF16)
    rank = jnp.dot(used.astype(BF16), earlier, preferred_element_type=F32)
    code = jnp.where(used, rank, -1.0)
    slot_of = lax.broadcasted_iota(jnp.int32, (EXPERTS, CAP, tokens), 1).astype(F32)
    match = code[:, None, :] == slot_of
    dispatch = match.astype(BF16).reshape(EXPERTS * CAP, tokens)
    combine = jnp.where(match, weight_of[:, None, :], 0.0).astype(BF16).reshape(EXPERTS * CAP, tokens)

    mixed = jnp.dot(regrouped, proj_weight, preferred_element_type=F32)
    hidden = residual_in.astype(F32) + mixed
    scale_rows = lax.rsqrt(jnp.mean(hidden * hidden, axis=-1, keepdims=True) + epsilon)
    normed = (hidden * scale_rows * norm_gain[None, :]).astype(BF16)
    width = normed.shape[1]
    buffer = jnp.dot(dispatch, normed, preferred_element_type=F32).astype(BF16)
    buffer = buffer.reshape(EXPERTS, CAP, width)
    slots = lax.all_to_all(buffer, "sp", split_axis=0, concat_axis=0, tiled=True).reshape(EXPERTS * CAP, width)
    gate_val = jnp.dot(slots, w_gate[0], preferred_element_type=F32)
    up_val = jnp.dot(slots, w_up[0], preferred_element_type=F32)
    act_rows = (jax.nn.silu(gate_val) * up_val).astype(BF16)
    expert_out = jnp.dot(act_rows, w_down[0], preferred_element_type=F32).astype(BF16)
    expert_out = expert_out.reshape(EXPERTS, CAP, width)
    returned = lax.all_to_all(expert_out, "sp", split_axis=0, concat_axis=0, tiled=True).reshape(EXPERTS * CAP, width)
    expert_sum = lax.dot_general(combine, returned, (((0,), (0,)), ((), ())), preferred_element_type=F32)
    return (hidden + expert_sum).astype(BF16)


def solution(mesh):
    return jax.shard_map(
        per_device,
        mesh=mesh,
        in_specs=(
            P(("sp", "tp"), None),
            P("sp", "tp"),
            P("sp", "tp"),
            P("sp", "tp"),
            P(None, "tp"),
            P("sp"),
            P(),
            P(),
            P(("sp", "tp"), None),
            P(("sp", "tp"), None),
            P("sp", None, None),
            P("sp", None, None),
            P("sp", None, None),
        ),
        out_specs=P(("sp", "tp"), None),
        check_vma=False,
    )
```

```python
import jax
import jax.numpy as jnp
from jax import lax
from jax.experimental import pallas as pl
from jax.experimental.pallas import tpu as pltpu
from jax.sharding import PartitionSpec as P

EXPERTS = 32
CAP = 64
epsilon = 1e-06
F32 = jnp.float32
BF16 = jnp.bfloat16
MESH = pl.DeviceIdType.MESH
HALF = 256


def from_behind(x, axis, by):
    devices = lax.axis_size(axis)
    pairs = [(i, i + by) for i in range(devices) if 0 <= i + by < devices]
    return lax.ppermute(x, axis, pairs)


class Copies:
    def __init__(self, send_sem, recv_sem):
        self.send_sem, self.recv_sem = send_sem, recv_sem
        self.made = {}
        self.unsent = []

    def start(self, name, src, dst, device):
        i = len(self.made)
        copy = pltpu.make_async_remote_copy(
            src_ref=src,
            dst_ref=dst,
            send_sem=self.send_sem.at[i],
            recv_sem=self.recv_sem.at[i],
            device_id=device,
            device_id_type=MESH,
        )
        self.made[name] = copy
        self.unsent.append(name)
        copy.start()

    def arrived(self, name):
        self.made[name].wait_recv()

    def sent(self, name):
        self.made[name].wait_send()
        self.unsent.remove(name)

    def finish(self):
        for name in list(self.unsent):
            self.sent(name)


COPIES = 64
LOCALS = 16


def layer_kernel(
    gated,
    residual,
    proj,
    gain,
    table,
    w_gate,
    w_up,
    w_down,
    out,
    all_gate,
    all_up,
    all_down,
    a2a,
    res_v,
    proj_v,
    gain_v,
    hidden,
    tok,
    tables,
    dispatch,
    combine,
    rows_x,
    rows_di,
    rows_in,
    act,
    outs,
    outs_far,
    returned,
    land,
    buf_gate,
    buf_up,
    buf_down,
    send_sem,
    recv_sem,
    local_sem,
):
    sp, tp = lax.axis_index("sp"), lax.axis_index("tp")
    z, y, c = sp // 8, (sp // 2) % 4, sp % 2
    width = tok.shape[2]
    rows = tok.shape[1]

    def place(yy, zz, cc):
        return zz * 8 + yy * 2 + cc

    y_in, z_in = y + 1 - 2 * (y % 2), z + 1 - 2 * (z % 2)
    near_y, near_z = (place(y_in, z, c), tp), (place(y, z_in, c), tp)
    far_y, far_z = (place(3 - y, z, c), tp), (place(y, 3 - z, c), tp)
    far_d = (place(3 - y, 3 - z, c), tp)
    other = (place(y, z, 1 - c), tp)
    right, left = (sp, (tp + 1) % 4), (sp, (tp + 3) % 4)
    across = (sp, (tp + 2) % 4)
    chips = [(y, z), (y_in, z), (y, z_in), (y_in, z_in)]
    expert_of = [place(yy, zz, cc) for yy, zz in chips for cc in (c, 1 - c)]

    barrier = pltpu.get_barrier_semaphore()
    partners = [near_y, near_z, far_y, far_z, far_d, other, right, left, across]
    for partner in partners:
        pl.semaphore_signal(barrier, inc=1, device_id=partner, device_id_type=MESH)
    pl.semaphore_wait(barrier, len(partners))

    cp = Copies(send_sem, recv_sem)
    fetches = {}

    def fetch(name, i, src, dst):
        fetches[name] = pltpu.make_async_copy(src, dst, local_sem.at[i])
        fetches[name].start()

    def strip(k):
        return pl.ds(pl.multiple_of(k * rows, rows), rows)

    for name, dev in (("r", right), ("l", left), ("a", across)):
        cp.start("mix_" + name, gated.at[strip(dev[1])], a2a.at[tp], dev)
    fetch("mix", 0, gated.at[strip(tp)], a2a.at[tp])
    fetch("proj", 1, proj, proj_v)
    fetch("res", 2, residual, res_v)
    fetch("gain", 3, gain, gain_v)
    fetch("table", 4, table, tables.at[0])
    mine = strip(tp)
    for name, dev, slot in (("y", near_y, 1), ("z", near_z, 3)):
        cp.start("gate_" + name, w_gate.at[mine], all_gate.at[slot, mine], dev)
    for name, dev, slot in (("y", near_y, 1), ("z", near_z, 3)):
        cp.start("up_" + name, w_up.at[mine], all_up.at[slot, mine], dev)
    for name, dev, slot in (("y", near_y, 1), ("z", near_z, 3)):
        cp.start("down_" + name, w_down, all_down.at[slot], dev)
    for name, dev, slot in (("y", far_y, 1), ("z", far_z, 2), ("d", far_d, 3)):
        cp.start("table_" + name, table, tables.at[slot], dev)
    cp.start("own_gate", w_gate, all_gate.at[0], other)
    cp.start("own_up", w_up, all_up.at[0], other)
    cp.start("own_down", w_down, all_down.at[0], other)

    for name in ("mix", "proj", "res", "gain"):
        fetches[name].wait()
    for name in ("r", "l", "a"):
        cp.arrived("mix_" + name)
    step = 512
    squares = jnp.zeros((rows, 1), F32)
    for n in range(0, width, step):
        part = res_v[:, n : n + step].astype(F32)
        for j in range(4):
            part = part + jnp.dot(a2a[j], proj_v[j * 256 : (j + 1) * 256, n : n + step], preferred_element_type=F32)
        hidden[:, n : n + step] = part
        squares = squares + jnp.sum(part * part, axis=1, keepdims=True)
    scale = lax.rsqrt(squares * (1.0 / width) + epsilon)
    for n in range(0, width, step):
        tok[0, :, n : n + step] = (hidden[:, n : n + step] * scale * gain_v[:, n : n + step]).astype(BF16)
    cp.start("tok_y", tok.at[0], tok.at[1], far_y)
    cp.start("tok_z", tok.at[0], tok.at[2], far_z)

    for kind, store in (("gate", all_gate), ("up", all_up)):
        for name, slot in (("y", 1), ("z", 3)):
            cp.arrived(kind + "_" + name)
            cp.start(kind + "_r_" + name, store.at[slot, mine], store.at[slot, mine], right)
            cp.start(kind + "_l_" + name, store.at[slot, mine], store.at[slot, mine], left)

    fetches["table"].wait()

    def matches(source, pair):
        slot = lax.broadcasted_iota(jnp.int32, (CAP, rows), 0).astype(F32)
        halves, weights = [], []
        for k in range(2):
            e = expert_of[2 * pair + k]
            hit = tables[source, pl.ds(e, 1), :] == slot
            halves.append(jnp.where(hit, 1.0, 0.0))
            weights.append(jnp.where(hit, tables[source, pl.ds(EXPERTS + e, 1), :], 0.0))
        return jnp.concatenate(halves, axis=0), jnp.concatenate(weights, axis=0)

    def gather(source, place_in, far):
        for pair in range(4):
            dispatch[pair * 128 : (pair + 1) * 128, :] = matches(source, pair)[0].astype(BF16)
        for n in range(0, width, step):
            got = jnp.dot(dispatch[...], tok[source, :, n : n + step], preferred_element_type=F32).astype(BF16)
            for e in range(6):
                rows_x[e, place_in * CAP : (place_in + 1) * CAP, n : n + step] = got[e * CAP : (e + 1) * CAP]
            rows_di[far, :, n : n + step] = got[6 * CAP :]

    def scatter(source, place_in, far, store):
        for pair in range(4):
            combine[:, pair * 128 : (pair + 1) * 128] = matches(source, pair)[1].T.astype(BF16)
        for n in range(0, width, step):
            total = jnp.dot(combine[:, :384], outs[place_in, :, n : n + step], preferred_element_type=F32)
            total = total + jnp.dot(combine[:, 384:], returned[far, :, n : n + step], preferred_element_type=F32)
            store(n, total)

    def load(e, slot):
        gate_from = w_gate if e == 0 else all_gate.at[e - 1]
        up_from = w_up if e == 0 else all_up.at[e - 1]
        down_from = w_down if e == 0 else all_down.at[e - 1]
        fetch(f"g{slot}", 5 + slot * 3, gate_from, buf_gate.at[slot])
        fetch(f"u{slot}", 6 + slot * 3, up_from, buf_up.at[slot])
        fetch(f"d{slot}", 7 + slot * 3, down_from, buf_down.at[slot])

    def feed_forward(e, slot, far):
        high = 128 if e < 2 else 192
        if e >= 2:
            far_in = far + 1 if e < 4 else far
            rows_x[e, 128:192, :] = rows_in[far_in, (e % 2) * CAP : (e % 2 + 1) * CAP, :]
        fetches[f"g{slot}"].wait()
        fetches[f"u{slot}"].wait()
        for n in range(0, 512, 256):
            left_side = rows_x[e, :high, :]
            gate_val = jnp.dot(left_side, buf_gate[slot, :, n : n + 256], preferred_element_type=F32)
            up_val = jnp.dot(left_side, buf_up[slot, :, n : n + 256], preferred_element_type=F32)
            act[:high, n : n + 256] = (gate_val / (1.0 + jnp.exp(-gate_val)) * up_val).astype(BF16)
        fetches[f"d{slot}"].wait()
        for n in range(0, width, step):
            got = jnp.dot(act[:high, :], buf_down[slot, :, n : n + step], preferred_element_type=F32).astype(BF16)
            for k in range(2):
                outs[k, e * CAP : (e + 1) * CAP, n : n + step] = got[k * CAP : (k + 1) * CAP]
            if e >= 2:
                far_in = far + 1 if e < 4 else far
                outs_far[far_in, (e % 2) * CAP : (e % 2 + 1) * CAP, n : n + step] = got[128:192]

    def ask(batch, k):
        dev = near_y if k == 0 else near_z
        cp.start(f"ask{batch}{k}", rows_di.at[2 * batch + k], rows_in.at[2 * batch + k], dev)

    def answer(batch, k):
        dev = near_y if k == 0 else near_z
        cp.start(f"ans{batch}{k}", outs_far.at[2 * batch + k], returned.at[2 * batch + k], dev)

    before, after = strip((tp + 3) % 4), strip((tp + 1) % 4)
    for name, slot in (("y", 1), ("z", 3)):
        cp.arrived("gate_r_" + name)
        cp.start("gate_f_" + name, all_gate.at[slot, before], all_gate.at[slot, before], right)
    for name, slot in (("y", 1), ("z", 3)):
        cp.arrived("up_l_" + name)
        cp.start("up_f_" + name, all_up.at[slot, after], all_up.at[slot, after], left)

    cp.arrived("tok_y")
    cp.arrived("tok_z")
    cp.start("tok_fy", tok.at[1, :HALF], tok.at[3, :HALF], far_z)
    cp.start("tok_fz", tok.at[2, HALF:], tok.at[3, HALF:], far_y)
    for name in ("y", "z", "d"):
        cp.arrived("table_" + name)

    gather(1, 0, 0)
    ask(0, 0)
    gather(2, 1, 1)
    ask(0, 1)
    for name in ("gate", "up", "down"):
        cp.arrived("own_" + name)
    load(0, 0)
    load(1, 1)
    feed_forward(0, 0, 0)
    for name, slot in (("y", 1), ("z", 3)):
        cp.arrived("down_" + name)
        cp.start("down_o_" + name, all_down.at[slot], all_down.at[slot + 1], other)
        cp.arrived("gate_l_" + name)
        cp.arrived("gate_f_" + name)
        cp.start("gate_o_" + name, all_gate.at[slot], all_gate.at[slot + 1], other)
        cp.arrived("up_r_" + name)
        cp.arrived("up_f_" + name)
        cp.start("up_o_" + name, all_up.at[slot], all_up.at[slot + 1], other)
    load(2, 0)
    feed_forward(1, 1, 0)
    cp.arrived("down_o_y")
    cp.arrived("gate_o_y")
    cp.arrived("up_o_y")
    load(3, 1)
    cp.arrived("ask01")
    feed_forward(2, 0, 0)
    load(4, 0)
    feed_forward(3, 1, 0)
    answer(0, 1)
    cp.arrived("down_o_z")
    cp.arrived("gate_o_z")
    cp.arrived("up_o_z")
    load(5, 1)
    cp.arrived("ask00")
    feed_forward(4, 0, 0)
    feed_forward(5, 1, 0)
    answer(0, 0)
    load(0, 0)
    load(1, 1)
    cp.arrived("tok_fy")
    cp.arrived("tok_fz")
    gather(0, 0, 2)
    ask(1, 0)
    gather(3, 1, 3)
    ask(1, 1)

    def into(k):
        def store(n, total):
            tok[k, :, n : n + step] = total.astype(BF16)

        return store

    cp.arrived("ans00")
    cp.sent("tok_fy")
    scatter(1, 0, 0, into(1))
    cp.start("pure_y", tok.at[1, :HALF], land.at[0], far_y)
    cp.arrived("ans01")
    cp.sent("tok_fz")
    scatter(2, 1, 1, into(2))
    cp.start("pure_z", tok.at[2, HALF:], land.at[1], far_z)

    feed_forward(0, 0, 2)
    load(2, 0)
    feed_forward(1, 1, 2)
    load(3, 1)
    cp.arrived("ask11")
    feed_forward(2, 0, 2)
    load(4, 0)
    feed_forward(3, 1, 2)
    answer(1, 1)
    load(5, 1)
    cp.arrived("ask10")
    feed_forward(4, 0, 2)
    feed_forward(5, 1, 2)
    answer(1, 0)
    cp.arrived("ans11")
    scatter(3, 1, 3, into(3))
    cp.start("diag_y", tok.at[3, :HALF], land.at[2], far_y)
    cp.start("diag_z", tok.at[3, HALF:], land.at[3], far_z)

    def onto_hidden(n, total):
        hidden[:, n : n + step] = hidden[:, n : n + step] + total

    cp.arrived("ans10")
    scatter(0, 0, 2, onto_hidden)

    cp.arrived("diag_y")
    tok[2, :HALF, :] = (tok[2, :HALF, :].astype(F32) + land[2].astype(F32)).astype(BF16)
    cp.start("fwd_z", tok.at[2, :HALF], land.at[4], far_z)
    cp.arrived("diag_z")
    tok[1, HALF:, :] = (tok[1, HALF:, :].astype(F32) + land[3].astype(F32)).astype(BF16)
    cp.start("fwd_y", tok.at[1, HALF:], land.at[5], far_y)
    cp.arrived("pure_y")
    hidden[:HALF, :] = hidden[:HALF, :] + land[0].astype(F32)
    cp.arrived("pure_z")
    hidden[HALF:, :] = hidden[HALF:, :] + land[1].astype(F32)
    cp.arrived("fwd_z")
    out[:HALF, :] = (hidden[:HALF, :] + land[4].astype(F32)).astype(BF16)
    cp.arrived("fwd_y")
    out[HALF:, :] = (hidden[HALF:, :] + land[5].astype(F32)).astype(BF16)
    cp.finish()


def layer(gated, residual, proj, gain, table, w_gate, w_up, w_down):
    rows, width = residual.shape
    hid = w_gate.shape[1]
    any_spec = pl.BlockSpec(memory_space=pl.ANY)
    shapes = (
        jax.ShapeDtypeStruct((rows, width), BF16),
        jax.ShapeDtypeStruct((5, width, hid), BF16),
        jax.ShapeDtypeStruct((5, width, hid), BF16),
        jax.ShapeDtypeStruct((5, hid, width), BF16),
    )
    return pl.pallas_call(
        layer_kernel,
        out_shape=shapes,
        in_specs=[any_spec] * 8,
        out_specs=(pl.BlockSpec(memory_space=pltpu.VMEM), any_spec, any_spec, any_spec),
        scratch_shapes=[
            pltpu.VMEM((4, rows, 256), BF16),
            pltpu.VMEM((rows, width), BF16),
            pltpu.VMEM((1024, width), BF16),
            pltpu.VMEM((1, width), F32),
            pltpu.VMEM((rows, width), F32),
            pltpu.VMEM((4, rows, width), BF16),
            pltpu.VMEM((4, 2 * EXPERTS, rows), F32),
            pltpu.VMEM((512, rows), BF16),
            pltpu.VMEM((rows, 512), BF16),
            pltpu.VMEM((6, 192, width), BF16),
            pltpu.VMEM((4, 128, width), BF16),
            pltpu.VMEM((4, 128, width), BF16),
            pltpu.VMEM((192, hid), BF16),
            pltpu.VMEM((2, 384, width), BF16),
            pltpu.VMEM((4, 128, width), BF16),
            pltpu.VMEM((4, 128, width), BF16),
            pltpu.VMEM((6, HALF, width), BF16),
            pltpu.VMEM((2, width, hid), BF16),
            pltpu.VMEM((2, width, hid), BF16),
            pltpu.VMEM((2, hid, width), BF16),
            pltpu.SemaphoreType.DMA((COPIES,)),
            pltpu.SemaphoreType.DMA((COPIES,)),
            pltpu.SemaphoreType.DMA((LOCALS,)),
        ],
        compiler_params=pltpu.CompilerParams(
            collective_id=0, has_side_effects=True, vmem_limit_bytes=67043328
        ),
        name="layer",
    )(gated, residual, proj, gain, table, w_gate, w_up, w_down)[0]


def per_device(
    residual_in,
    conv_input,
    input_gate,
    output_gate,
    conv_taps,
    doc_ids,
    proj_weight,
    norm_gain,
    expert_ids,
    expert_weight,
    w_gate,
    w_up,
    w_down,
):
    kernel_width = conv_taps.shape[0]
    rim = kernel_width - 1
    length, channels = conv_input.shape
    doc_float = doc_ids.astype(F32)
    tail = input_gate[-rim:].astype(F32) * conv_input[-rim:].astype(F32)
    packed = jnp.concatenate([tail, jnp.broadcast_to(doc_float[-rim:, None], (rim, 128))], axis=1)
    prev = from_behind(packed, "sp", 1)
    prev_in, prev_ids = prev[:, :channels], prev[:, channels]
    product = input_gate.astype(F32) * conv_input.astype(F32)
    padded_in = jnp.concatenate([prev_in, product], axis=0)
    padded_ids = jnp.concatenate([prev_ids, doc_float], axis=0)
    conv_sum = jnp.zeros(product.shape, F32)
    for offset in range(kernel_width):
        same_doc = padded_ids[offset : offset + length] == doc_float
        term = conv_taps[offset].astype(F32)[None, :] * padded_in[offset : offset + length]
        conv_sum = conv_sum + jnp.where(same_doc[:, None], term, 0.0)
    gated = (output_gate.astype(F32) * conv_sum).astype(BF16)

    tokens = expert_ids.shape[0]
    experts = jnp.arange(EXPERTS, dtype=jnp.int32)
    ids_t = expert_ids.T
    weight_t = expert_weight.T
    hit = [ids_t[j][None, :] == experts[:, None] for j in range(2)]
    used = hit[0] | hit[1]
    weight_of = jnp.where(hit[0], weight_t[0][None, :], 0.0) + jnp.where(hit[1], weight_t[1][None, :], 0.0)
    t_row = lax.broadcasted_iota(jnp.int32, (tokens, tokens), 0)
    t_col = lax.broadcasted_iota(jnp.int32, (tokens, tokens), 1)
    earlier = (t_row < t_col).astype(BF16)
    rank = jnp.dot(used.astype(BF16), earlier, preferred_element_type=F32)
    code = jnp.where(used, rank, -1.0)
    table = jnp.concatenate([code, weight_of], axis=0)
    return layer(
        gated, residual_in, proj_weight, norm_gain[None, :], table, w_gate[0], w_up[0], w_down[0]
    )


def solution(mesh):
    return jax.shard_map(
        per_device,
        mesh=mesh,
        in_specs=(
            P(("sp", "tp"), None),
            P("sp", "tp"),
            P("sp", "tp"),
            P("sp", "tp"),
            P(None, "tp"),
            P("sp"),
            P(),
            P(),
            P(("sp", "tp"), None),
            P(("sp", "tp"), None),
            P("sp", None, None),
            P("sp", None, None),
            P("sp", None, None),
        ),
        out_specs=P(("sp", "tp"), None),
        check_vma=False,
    )
```

```python
import jax
import jax.numpy as jnp
from jax import lax
from jax.experimental import pallas as pl
from jax.experimental.pallas import tpu as pltpu
from jax.sharding import PartitionSpec as P

EXPERTS = 32
CAP = 64
epsilon = 1e-06
F32 = jnp.float32
BF16 = jnp.bfloat16
MESH = pl.DeviceIdType.MESH
HALF = 256
DIRECT = 128


class Copies:
    def __init__(self, send_sem, recv_sem):
        self.send_sem, self.recv_sem = send_sem, recv_sem
        self.made = {}
        self.unsent = []

    def start(self, name, src, dst, device):
        i = len(self.made)
        copy = pltpu.make_async_remote_copy(
            src_ref=src,
            dst_ref=dst,
            send_sem=self.send_sem.at[i],
            recv_sem=self.recv_sem.at[i],
            device_id=device,
            device_id_type=MESH,
        )
        self.made[name] = copy
        self.unsent.append(name)
        copy.start()

    def arrived(self, name):
        self.made[name].wait_recv()

    def sent(self, name):
        self.made[name].wait_send()
        self.unsent.remove(name)

    def finish(self):
        for name in list(self.unsent):
            self.sent(name)


COPIES = 96
LOCALS = 24
A_COLS, B_COLS = slice(0, 1024), slice(1024, 2048)


def layer_kernel(
    residual,
    conv_input,
    input_gate,
    output_gate,
    taps,
    docs,
    proj,
    gain,
    ids,
    route_weight,
    w_gate,
    w_up,
    w_down,
    hidden_out,
    far_out,
    all_gate,
    all_up,
    all_down,
    taps_v,
    docs_v,
    ids_v,
    route_v,
    halo_c,
    halo_g,
    halo_d,
    product,
    doc_rows,
    gated,
    a2a,
    gain_v,
    hidden,
    tok,
    tables,
    dispatch,
    combine,
    rows_x,
    rows_di,
    rows_in,
    act,
    outs,
    outs_far,
    returned,
    land,
    buf_gate,
    buf_up,
    buf_down,
    send_sem,
    recv_sem,
    local_sem,
):
    sp, tp = lax.axis_index("sp"), lax.axis_index("tp")
    z, y, c = sp // 8, (sp // 2) % 4, sp % 2
    rows, width = tok.shape[1], tok.shape[2]
    length = gated.shape[0]

    def place(yy, zz, cc):
        return zz * 8 + yy * 2 + cc

    y_in, z_in = y + 1 - 2 * (y % 2), z + 1 - 2 * (z % 2)
    near_y, near_z = (place(y_in, z, c), tp), (place(y, z_in, c), tp)
    far_y, far_z = (place(3 - y, z, c), tp), (place(y, 3 - z, c), tp)
    far_d = (place(3 - y, 3 - z, c), tp)
    other = (place(y, z, 1 - c), tp)
    right, left = (sp, (tp + 1) % 4), (sp, (tp + 3) % 4)
    across = (sp, (tp + 2) % 4)
    ahead, behind = ((sp + 1) % 32, tp), ((sp + 31) % 32, tp)
    chips = [(y, z), (y_in, z), (y, z_in), (y_in, z_in)]
    expert_of = [place(yy, zz, cc) for yy, zz in chips for cc in (c, 1 - c)]

    barrier = pltpu.get_barrier_semaphore()
    partners = [near_y, near_z, far_y, far_z, far_d, other, right, left, across, ahead, behind]
    for partner in partners:
        pl.semaphore_signal(barrier, inc=1, device_id=partner, device_id_type=MESH)

    cp = Copies(send_sem, recv_sem)
    fetches = {}

    def fetch(name, src, dst, i=None):
        i = 9 + len(fetches) if i is None else i
        fetches[name] = pltpu.make_async_copy(src, dst, local_sem.at[i])
        fetches[name].start()

    def strip(k):
        return pl.ds(pl.multiple_of(k * rows, rows), rows)

    conv_v, in_gate_v = buf_gate.at[0, :, :256], buf_gate.at[0, :, 256:]
    out_gate_v = buf_gate.at[1, :, :256]
    fetch("conv", conv_input, conv_v)
    fetch("in_gate", input_gate, in_gate_v)
    fetch("out_gate", output_gate, out_gate_v)
    fetch("taps", taps, taps_v)
    fetch("docs", docs, docs_v)
    fetch("ids", ids, ids_v)
    fetch("route", route_weight, route_v)
    fetch("gain", gain, gain_v)
    fetch("proj0", proj.at[:512], buf_down.at[0])
    fetch("proj1", proj.at[512:], buf_down.at[1])
    fetch("res0", residual.at[:256], rows_x.at[0])
    fetch("res1", residual.at[256:], rows_x.at[1])
    pl.semaphore_wait(barrier, len(partners))

    cp.start("halo_c", conv_input.at[length - 16 :], halo_c, ahead)
    cp.start("halo_g", input_gate.at[length - 16 :], halo_g, ahead)
    cp.start("halo_d", docs.at[8:], halo_d, ahead)
    mine = strip(tp)
    near = (("y", near_y, 1), ("z", near_z, 3))
    for name, dev, slot in near:
        cp.start("gate_" + name, w_gate.at[mine], all_gate.at[slot, mine], dev)
    for name, dev, slot in near:
        cp.start("up_" + name, w_up.at[mine], all_up.at[slot, mine], dev)
    late = pl.ds(pl.multiple_of(((tp + 2) % 4) * rows + rows - DIRECT, DIRECT), DIRECT)
    cp.start("gate_d_y", w_gate.at[late], all_gate.at[1, late], near_y)
    cp.start("up_d_z", w_up.at[late], all_up.at[3, late], near_z)
    for name, dev, slot in near:
        cp.start("down_" + name, w_down, all_down.at[slot], dev)
    cp.start("own_gate", w_gate, all_gate.at[0], other)
    cp.start("own_up", w_up, all_up.at[0], other)
    cp.start("own_down", w_down, all_down.at[0], other)

    for name in ("conv", "in_gate", "out_gate", "taps", "docs"):
        fetches[name].wait()
    for r in range(length // 128):
        doc_rows[8 + r * 128 : 136 + r * 128, :] = jnp.broadcast_to(
            docs_v[r : r + 1, :].astype(F32), (128, 128)
        ).T
    for r in range(0, length, 256):
        product[8 + r : 264 + r, :] = buf_gate[0, r : r + 256, :256].astype(F32) * buf_gate[
            0, r : r + 256, 256:
        ].astype(F32)
    tap = [taps_v[k : k + 1, :].astype(F32) for k in range(3)]

    def convolve(r):
        here = doc_rows[8 + r : 264 + r, :]
        same = [doc_rows[6 + k + r : 262 + k + r, :] == here for k in range(2)]
        for h in (0, 128):
            total = tap[2][:, h : h + 128] * product[8 + r : 264 + r, h : h + 128]
            for k in range(2):
                term = tap[k][:, h : h + 128] * product[6 + k + r : 262 + k + r, h : h + 128]
                total = total + jnp.where(same[k], term, 0.0)
            gated[r : r + 256, h : h + 128] = (
                buf_gate[1, r : r + 256, h : h + 128].astype(F32) * total
            ).astype(BF16)

    for r in range(256, length, 256):
        convolve(r)
    cp.arrived("halo_c")
    cp.arrived("halo_g")
    cp.arrived("halo_d")
    product[:8, :] = (halo_c[...].astype(F32) * halo_g[...].astype(F32))[8:]
    halo_docs = jnp.broadcast_to(halo_d[7:8, :].astype(F32), (128, 128)).T
    doc_rows[:8, :] = jnp.where(sp == 0, -1.0, halo_docs[120:])
    convolve(0)

    for name, dev in (("r", right), ("l", left), ("a", across)):
        cp.start("mix_" + name, gated.at[strip(dev[1])], a2a.at[tp], dev)
    fetch("mix", gated.at[strip(tp)], a2a.at[tp])

    def share(kind, name, part, at):
        store = all_gate if kind == "gate" else all_up
        slot = 1 if name == "y" else 3
        cp.start(f"{kind}_o{part}_{name}", store.at[slot, at], store.at[slot + 1, at], other)

    def turn(kind, way, name, part, at):
        store = all_gate if kind == "gate" else all_up
        slot = 1 if name == "y" else 3
        cp.start(
            f"{kind}_{part}_{name}", store.at[slot, at], store.at[slot, at], right if way == "r" else left
        )

    before, after, opposite = strip((tp + 3) % 4), strip((tp + 1) % 4), strip((tp + 2) % 4)

    def early(k):
        return pl.ds(pl.multiple_of((k % 4) * rows, rows), rows - DIRECT)

    for name in ("y", "z"):
        cp.arrived("gate_" + name)
        turn("gate", "r", name, "r", mine)
        turn("gate", "l", name, "l", mine)
        share("gate", name, "m", mine)

    fetches["ids"].wait()
    fetches["route"].wait()
    experts = lax.broadcasted_iota(jnp.int32, (EXPERTS, rows), 0)
    hit = [ids_v[j : j + 1, :] == experts for j in range(2)]
    used = jnp.where(hit[0], 1.0, jnp.where(hit[1], 1.0, 0.0))
    earlier = lax.broadcasted_iota(jnp.int32, (rows, rows), 0) < lax.broadcasted_iota(jnp.int32, (rows, rows), 1)
    dispatch[...] = jnp.where(earlier, 1.0, 0.0).astype(BF16)
    rank = jnp.dot(used.astype(BF16), dispatch[...], preferred_element_type=F32)
    tables[0, :EXPERTS, :] = jnp.where(used > 0.0, rank, -1.0)
    tables[0, EXPERTS:, :] = jnp.where(hit[0], route_v[0:1, :], jnp.where(hit[1], route_v[1:2, :], 0.0))

    for name, dev, slot in (("y", far_y, 1), ("z", far_z, 2), ("d", far_d, 3)):
        cp.start("table_" + name, tables.at[0], tables.at[slot], dev)

    for name in ("mix", "proj0", "proj1", "res0", "res1", "gain"):
        fetches[name].wait()
    for name in ("r", "l", "a"):
        cp.arrived("mix_" + name)
    step = 512

    def project():
        squares = jnp.zeros((rows, 1), F32)
        for n in range(0, width, step):
            part = jnp.concatenate([rows_x[0, :, n : n + step], rows_x[1, :, n : n + step]], axis=0).astype(F32)
            for j in range(4):
                part = part + jnp.dot(
                    a2a[j],
                    buf_down[j // 2, (j % 2) * 256 : (j % 2 + 1) * 256, n : n + step],
                    preferred_element_type=F32,
                )
            hidden[:, n : n + step] = part
            squares = squares + jnp.sum(part * part, axis=1, keepdims=True)
        scale = lax.rsqrt(squares * (1.0 / width) + epsilon)
        for n in range(0, width, step):
            tok[0, :, n : n + step] = (hidden[:, n : n + step] * scale * gain_v[:, n : n + step]).astype(BF16)

    project()
    cp.start("tok_y", tok.at[0], tok.at[1], far_y)
    cp.start("tok_z", tok.at[0], tok.at[2], far_z)

    def matches(source, pair):
        slot = lax.broadcasted_iota(jnp.int32, (CAP, rows), 0).astype(F32)
        halves, weights = [], []
        for k in range(2):
            e = expert_of[2 * pair + k]
            same = tables[source, pl.ds(e, 1), :] == slot
            halves.append(jnp.where(same, 1.0, 0.0))
            weights.append(jnp.where(same, tables[source, pl.ds(EXPERTS + e, 1), :], 0.0))
        return jnp.concatenate(halves, axis=0), jnp.concatenate(weights, axis=0)

    source_of = [1, 2, 0, 3]

    def gather(i):
        source = source_of[i]
        for pair in range(4):
            dispatch[pair * 128 : (pair + 1) * 128, :] = matches(source, pair)[0].astype(BF16)
        for n in range(0, width, step):
            got = jnp.dot(dispatch[...], tok[source, :, n : n + step], preferred_element_type=F32).astype(BF16)
            for e in range(6):
                rows_x[e, i * CAP : (i + 1) * CAP, n : n + step] = got[e * CAP : (e + 1) * CAP]
            rows_di[i, :, n : n + step] = got[6 * CAP :]

    def weigh(i):
        for pair in range(4):
            combine[:, pair * 128 : (pair + 1) * 128] = matches(source_of[i], pair)[1].T.astype(BF16)

    def scatter(i, cols, store):
        for n in range(cols.start, cols.stop, step):
            total = jnp.dot(combine[:, :384], outs[i, :, n : n + step], preferred_element_type=F32)
            total = total + jnp.dot(combine[:, 384:], returned[i, :, n : n + step], preferred_element_type=F32)
            store(n, total)

    def load(e, slot):
        gate_from = w_gate if e == 0 else all_gate.at[e - 1]
        up_from = w_up if e == 0 else all_up.at[e - 1]
        down_from = w_down if e == 0 else all_down.at[e - 1]
        fetch(f"g{slot}", gate_from, buf_gate.at[slot], slot * 3)
        fetch(f"u{slot}", up_from, buf_up.at[slot], slot * 3 + 1)
        fetch(f"d{slot}", down_from, buf_down.at[slot], slot * 3 + 2)

    def loaded(slot):
        for kind in "gud":
            fetches[f"{kind}{slot}"].wait()

    def activate(slot, left_ref, high):
        for n in range(0, 512, 256):
            left_side = left_ref[...]
            gate_val = jnp.dot(left_side, buf_gate[slot, :, n : n + 256], preferred_element_type=F32)
            up_val = jnp.dot(left_side, buf_up[slot, :, n : n + 256], preferred_element_type=F32)
            act[:high, n : n + 256] = (gate_val / (1.0 + jnp.exp(-gate_val)) * up_val).astype(BF16)

    def local(e, slot, batch):
        activate(slot, rows_x.at[e, batch * 128 : (batch + 1) * 128], 128)
        for n in range(0, width, step):
            got = jnp.dot(act[...], buf_down[slot, :, n : n + step], preferred_element_type=F32).astype(BF16)
            for k in range(2):
                outs[2 * batch + k, e * CAP : (e + 1) * CAP, n : n + step] = got[k * CAP : (k + 1) * CAP]

    def distant(e, slot, i):
        at = slice((e % 2) * CAP, (e % 2 + 1) * CAP)
        activate(slot, rows_in.at[i, at], CAP)
        for n in range(0, width, step):
            outs_far[i, at, n : n + step] = jnp.dot(
                act[:CAP, :], buf_down[slot, :, n : n + step], preferred_element_type=F32
            ).astype(BF16)

    def ask(i):
        cp.start(f"ask{i}", rows_di.at[i], rows_in.at[i], near_y if i % 2 == 0 else near_z)

    def answer(e, i, order):
        at = slice((e % 2) * CAP, (e % 2 + 1) * CAP)
        for half in order:
            cols = A_COLS if half == "a" else B_COLS
            cp.start(
                f"ans{i}{e % 2}{half}",
                outs_far.at[i, at, cols],
                returned.at[i, at, cols],
                near_y if i % 2 == 0 else near_z,
            )

    def answered(i, half):
        for k in range(2):
            cp.arrived(f"ans{i}{k}{half}")

    gather(2)
    cp.arrived("up_y")
    turn("up", "r", "y", "r", mine)
    turn("up", "l", "y", "l", mine)
    share("up", "y", "m", mine)
    cp.arrived("gate_r_y")
    turn("gate", "r", "y", "f", early(tp + 3))
    share("gate", "y", "r", before)
    cp.arrived("up_z")
    turn("up", "r", "z", "r", mine)
    share("up", "z", "m", mine)
    cp.arrived("gate_l_y")
    share("gate", "y", "l", after)
    cp.arrived("gate_r_z")
    turn("gate", "r", "z", "f", before)
    share("gate", "z", "r", before)
    cp.arrived("up_d_z")
    share("up", "z", "d", late)
    cp.arrived("gate_l_z")
    share("gate", "z", "l", after)
    cp.arrived("up_l_y")
    turn("up", "l", "y", "f", after)
    turn("up", "l", "z", "l", mine)
    share("up", "y", "l", after)
    cp.arrived("up_r_y")
    share("up", "y", "r", before)
    for name in ("gate", "up", "down"):
        cp.arrived("own_" + name)
    load(0, 0)
    load(1, 1)
    cp.arrived("gate_f_y")
    share("gate", "y", "f", early(tp + 2))
    cp.arrived("gate_d_y")
    share("gate", "y", "d", late)
    cp.arrived("up_f_y")
    share("up", "y", "f", opposite)

    cp.arrived("tok_y")
    cp.start("tok_fy", tok.at[1, :HALF], tok.at[3, :HALF], far_z)
    cp.arrived("tok_z")
    cp.start("tok_fz", tok.at[2, HALF:], tok.at[3, HALF:], far_y)
    cp.arrived("table_y")
    gather(0)
    ask(0)
    cp.arrived("table_z")
    gather(1)
    ask(1)

    cp.arrived("down_y")
    cp.start("down_o_y", all_down.at[1], all_down.at[2], other)
    load(2, 2)
    cp.arrived("up_l_z")
    turn("up", "l", "z", "f", early(tp + 1))
    share("up", "z", "l", after)
    loaded(0)
    local(0, 0, 0)
    for kind, parts in (("gate", "mrlfd"), ("up", "mrlf")):
        for part in parts:
            cp.arrived(f"{kind}_o{part}_y")
    loaded(1)
    local(1, 1, 0)
    cp.arrived("down_o_y")
    load(3, 0)
    cp.arrived("up_r_z")
    share("up", "z", "r", before)
    cp.arrived("down_z")
    cp.start("down_o_z", all_down.at[3], all_down.at[4], other)
    loaded(2)
    local(2, 2, 0)
    loaded(0)
    local(3, 0, 0)
    cp.arrived("gate_f_z")
    share("gate", "z", "f", opposite)
    cp.arrived("up_f_z")
    share("up", "z", "f", early(tp + 2))
    load(4, 1)
    cp.arrived("ask1")
    distant(2, 2, 1)
    answer(2, 1, "b")
    distant(3, 0, 1)
    answer(3, 1, "b")
    answer(2, 1, "a")
    answer(3, 1, "a")
    for kind, parts in (("gate", "mrlf"), ("up", "mrlfd")):
        for part in parts:
            cp.arrived(f"{kind}_o{part}_z")
    cp.arrived("down_o_z")
    load(5, 2)
    cp.arrived("ask0")
    loaded(1)
    distant(4, 1, 0)
    answer(4, 0, "a")
    loaded(2)
    distant(5, 2, 0)
    answer(5, 0, "a")
    answer(4, 0, "b")
    answer(5, 0, "b")
    ask(2)
    local(4, 1, 0)
    local(5, 2, 0)

    def into(k):
        def store(n, total):
            tok[k, :, n : n + step] = total.astype(BF16)

        return store

    cp.sent("tok_fz")
    weigh(1)
    answered(1, "b")
    scatter(1, B_COLS, into(2))
    cp.start("pure_z", tok.at[2, :, B_COLS], land.at[1], far_z)
    cp.arrived("tok_fy")
    cp.arrived("tok_fz")
    cp.arrived("table_d")
    gather(3)
    ask(3)
    cp.sent("tok_fy")
    weigh(0)
    answered(0, "a")
    scatter(0, A_COLS, into(1))
    cp.start("pure_y", tok.at[1, :, A_COLS], land.at[0], far_y)

    local(5, 2, 1)
    load(0, 2)
    local(4, 1, 1)
    answered(0, "b")
    scatter(0, B_COLS, into(1))
    loaded(2)
    local(0, 2, 1)
    load(1, 2)
    weigh(1)
    answered(1, "a")
    scatter(1, A_COLS, into(2))
    loaded(2)
    local(1, 2, 1)
    load(2, 2)
    cp.arrived("ask3")
    distant(3, 0, 3)
    answer(3, 3, "b")
    loaded(2)
    distant(2, 2, 3)
    answer(2, 3, "ba")
    answer(3, 3, "a")
    local(3, 0, 1)
    load(5, 0)
    local(2, 2, 1)
    weigh(3)
    cp.arrived("ask2")
    distant(4, 1, 2)
    answer(4, 2, "ab")
    answered(3, "b")
    scatter(3, B_COLS, into(3))
    for r in range(2):
        at = slice(r * HALF, (r + 1) * HALF)
        cp.start(f"diag_z{r}", tok.at[3, at, B_COLS], land.at[3, at], far_z)
    answered(3, "a")
    scatter(3, A_COLS, into(3))
    for r in range(2):
        at = slice(r * HALF, (r + 1) * HALF)
        cp.start(f"diag_y{r}", tok.at[3, at, A_COLS], land.at[2, at], far_y)
    loaded(0)
    distant(5, 0, 2)
    answer(5, 2, "ab")

    def onto_hidden(n, total):
        hidden[:, n : n + step] = hidden[:, n : n + step] + total

    weigh(2)
    answered(2, "a")
    answered(2, "b")
    scatter(2, A_COLS, onto_hidden)
    scatter(2, B_COLS, onto_hidden)
    cp.arrived("pure_z")
    hidden[:, B_COLS] = hidden[:, B_COLS] + land[1].astype(F32)
    cp.arrived("pure_y")
    hidden[:, A_COLS] = hidden[:, A_COLS] + land[0].astype(F32)
    fetch("hidden", hidden, hidden_out)

    for r in range(2):
        at = slice(r * HALF, (r + 1) * HALF)
        cp.arrived(f"diag_z{r}")
        tok[1, at, B_COLS] = (tok[1, at, B_COLS].astype(F32) + land[3, at].astype(F32)).astype(BF16)
        cp.start(f"fwd_y{r}", tok.at[1, at, B_COLS], far_out.at[at, B_COLS], far_y)
        cp.arrived(f"diag_y{r}")
        tok[2, at, A_COLS] = (tok[2, at, A_COLS].astype(F32) + land[2, at].astype(F32)).astype(BF16)
        cp.start(f"fwd_z{r}", tok.at[2, at, A_COLS], far_out.at[at, A_COLS], far_z)
    fetches["hidden"].wait()
    for r in range(2):
        cp.arrived(f"fwd_z{r}")
        cp.arrived(f"fwd_y{r}")
    cp.finish()


def layer(*operands):
    residual, w_gate = operands[0], operands[10]
    rows, width = residual.shape
    hid = w_gate.shape[1]
    length, channels = operands[1].shape
    any_spec = pl.BlockSpec(memory_space=pl.ANY)
    shapes = (
        jax.ShapeDtypeStruct((rows, width), F32),
        jax.ShapeDtypeStruct((rows, width), BF16),
        jax.ShapeDtypeStruct((5, width, hid), BF16),
        jax.ShapeDtypeStruct((5, width, hid), BF16),
        jax.ShapeDtypeStruct((5, hid, width), BF16),
    )
    hidden, far = pl.pallas_call(
        layer_kernel,
        out_shape=shapes,
        in_specs=[any_spec] * len(operands),
        out_specs=(any_spec,) * 5,
        scratch_shapes=[
            pltpu.VMEM((3, channels), BF16),
            pltpu.VMEM((length // 128, 128), jnp.int32),
            pltpu.VMEM((2, rows), jnp.int32),
            pltpu.VMEM((2, rows), F32),
            pltpu.VMEM((16, channels), BF16),
            pltpu.VMEM((16, channels), BF16),
            pltpu.VMEM((8, 128), jnp.int32),
            pltpu.VMEM((length + 8, channels), F32),
            pltpu.VMEM((length + 8, 128), F32),
            pltpu.VMEM((length, channels), BF16),
            pltpu.VMEM((4, rows, channels), BF16),
            pltpu.VMEM((1, width), F32),
            pltpu.VMEM((rows, width), F32),
            pltpu.VMEM((4, rows, width), BF16),
            pltpu.VMEM((4, 2 * EXPERTS, rows), F32),
            pltpu.VMEM((512, rows), BF16),
            pltpu.VMEM((rows, 512), BF16),
            pltpu.VMEM((6, 256, width), BF16),
            pltpu.VMEM((4, 128, width), BF16),
            pltpu.VMEM((4, 128, width), BF16),
            pltpu.VMEM((128, hid), BF16),
            pltpu.VMEM((4, 384, width), BF16),
            pltpu.VMEM((4, 128, width), BF16),
            pltpu.VMEM((4, 128, width), BF16),
            pltpu.VMEM((4, rows, width // 2), BF16),
            pltpu.VMEM((3, width, hid), BF16),
            pltpu.VMEM((3, width, hid), BF16),
            pltpu.VMEM((3, hid, width), BF16),
            pltpu.SemaphoreType.DMA((COPIES,)),
            pltpu.SemaphoreType.DMA((COPIES,)),
            pltpu.SemaphoreType.DMA((LOCALS + 16,)),
        ],
        compiler_params=pltpu.CompilerParams(
            collective_id=0, has_side_effects=True, vmem_limit_bytes=67043328
        ),
        name="layer",
    )(*operands)[:2]
    return (hidden + far.astype(F32)).astype(BF16)


def per_device(
    residual_in,
    conv_input,
    input_gate,
    output_gate,
    conv_taps,
    doc_ids,
    proj_weight,
    norm_gain,
    expert_ids,
    expert_weight,
    w_gate,
    w_up,
    w_down,
):
    return layer(
        residual_in,
        conv_input,
        input_gate,
        output_gate,
        conv_taps,
        doc_ids.reshape(-1, 128),
        proj_weight,
        norm_gain[None, :],
        expert_ids.T,
        expert_weight.T,
        w_gate[0],
        w_up[0],
        w_down[0],
    )


def solution(mesh):
    return jax.shard_map(
        per_device,
        mesh=mesh,
        in_specs=(
            P(("sp", "tp"), None),
            P("sp", "tp"),
            P("sp", "tp"),
            P("sp", "tp"),
            P(None, "tp"),
            P("sp"),
            P(),
            P(),
            P(("sp", "tp"), None),
            P(("sp", "tp"), None),
            P("sp", None, None),
            P("sp", None, None),
            P("sp", None, None),
        ),
        out_specs=P(("sp", "tp"), None),
        check_vma=False,
    )
```

```python
import jax
import jax.numpy as jnp
from jax import lax
from jax.experimental import pallas as pl
from jax.experimental.pallas import tpu as pltpu
from jax.sharding import PartitionSpec as P

EXPERTS = 32
CAP = 64
epsilon = 1e-06
F32 = jnp.float32
BF16 = jnp.bfloat16
MESH = pl.DeviceIdType.MESH
HALF = 256
DIRECT = 128


class Copies:
    def __init__(self, send_sem, recv_sem):
        self.send_sem, self.recv_sem = send_sem, recv_sem
        self.made = {}
        self.unsent = []

    def start(self, name, src, dst, device):
        i = len(self.made)
        copy = pltpu.make_async_remote_copy(
            src_ref=src,
            dst_ref=dst,
            send_sem=self.send_sem.at[i],
            recv_sem=self.recv_sem.at[i],
            device_id=device,
            device_id_type=MESH,
        )
        self.made[name] = copy
        self.unsent.append(name)
        copy.start()

    def arrived(self, name):
        self.made[name].wait_recv()

    def sent(self, name):
        self.made[name].wait_send()
        self.unsent.remove(name)

    def finish(self):
        for name in list(self.unsent):
            self.sent(name)


COPIES = 112
LOCALS = 24
A_COLS, B_COLS = slice(0, 1024), slice(1024, 2048)


def layer_kernel(
    residual,
    conv_input,
    input_gate,
    output_gate,
    taps,
    docs,
    proj,
    gain,
    ids,
    route_weight,
    w_gate,
    w_up,
    w_down,
    hidden_out,
    far_out,
    all_gate,
    all_up,
    all_down,
    taps_v,
    docs_v,
    ids_v,
    route_v,
    halo_c,
    halo_g,
    halo_d,
    product,
    doc_rows,
    gated,
    a2a,
    gain_v,
    hidden,
    tok,
    tables,
    dispatch,
    combine,
    rows_x,
    rows_di,
    rows_in,
    act,
    outs,
    outs_far,
    returned,
    land,
    buf_gate,
    buf_up,
    buf_down,
    send_sem,
    recv_sem,
    local_sem,
):
    sp, tp = lax.axis_index("sp"), lax.axis_index("tp")
    z, y, c = sp // 8, (sp // 2) % 4, sp % 2
    rows, width = tok.shape[1], tok.shape[2]
    length = gated.shape[0]

    def place(yy, zz, cc):
        return zz * 8 + yy * 2 + cc

    y_in, z_in = y + 1 - 2 * (y % 2), z + 1 - 2 * (z % 2)
    near_y, near_z = (place(y_in, z, c), tp), (place(y, z_in, c), tp)
    far_y, far_z = (place(3 - y, z, c), tp), (place(y, 3 - z, c), tp)
    far_d = (place(3 - y, 3 - z, c), tp)
    other = (place(y, z, 1 - c), tp)
    right, left = (sp, (tp + 1) % 4), (sp, (tp + 3) % 4)
    across = (sp, (tp + 2) % 4)
    ahead, behind = ((sp + 1) % 32, tp), ((sp + 31) % 32, tp)
    chips = [(y, z), (y_in, z), (y, z_in), (y_in, z_in)]
    expert_of = [place(yy, zz, cc) for yy, zz in chips for cc in (c, 1 - c)]

    barrier = pltpu.get_barrier_semaphore()
    partners = [near_y, near_z, far_y, far_z, far_d, other, right, left, across, ahead, behind]
    for partner in partners:
        pl.semaphore_signal(barrier, inc=1, device_id=partner, device_id_type=MESH)

    cp = Copies(send_sem, recv_sem)
    fetches = {}

    def fetch(name, src, dst, i=None):
        i = 9 + len(fetches) if i is None else i
        fetches[name] = pltpu.make_async_copy(src, dst, local_sem.at[i])
        fetches[name].start()

    def strip(k):
        return pl.ds(pl.multiple_of(k * rows, rows), rows)

    conv_v, in_gate_v = buf_gate.at[0, :, :256], buf_gate.at[0, :, 256:]
    out_gate_v = buf_gate.at[1, :, :256]
    fetch("conv", conv_input, conv_v)
    fetch("in_gate", input_gate, in_gate_v)
    fetch("out_gate", output_gate, out_gate_v)
    fetch("taps", taps, taps_v)
    fetch("docs", docs, docs_v)
    fetch("ids", ids, ids_v)
    fetch("route", route_weight, route_v)
    fetch("gain", gain, gain_v)
    fetch("proj0", proj.at[:512], buf_down.at[0])
    fetch("proj1", proj.at[512:], buf_down.at[1])
    fetch("res0", residual.at[:256], rows_x.at[0])
    fetch("res1", residual.at[256:], rows_x.at[1])
    pl.semaphore_wait(barrier, len(partners))

    cp.start("halo_c", conv_input.at[length - 16 :], halo_c, ahead)
    cp.start("halo_g", input_gate.at[length - 16 :], halo_g, ahead)
    cp.start("halo_d", docs.at[8:], halo_d, ahead)
    mine = strip(tp)
    near = (("y", near_y, 1), ("z", near_z, 3))
    for name, dev, slot in near:
        cp.start("gate_" + name, w_gate.at[mine], all_gate.at[slot, mine], dev)
    for name, dev, slot in near:
        cp.start("up_" + name, w_up.at[mine], all_up.at[slot, mine], dev)
    late = pl.ds(pl.multiple_of(((tp + 2) % 4) * rows + rows - DIRECT, DIRECT), DIRECT)
    cp.start("gate_d_y", w_gate.at[late], all_gate.at[1, late], near_y)
    cp.start("up_d_z", w_up.at[late], all_up.at[3, late], near_z)
    for name, dev, slot in near:
        cp.start("down_" + name, w_down, all_down.at[slot], dev)
    cp.start("own_gate", w_gate, all_gate.at[0], other)
    cp.start("own_up", w_up, all_up.at[0], other)
    cp.start("own_down", w_down, all_down.at[0], other)

    for name in ("conv", "in_gate", "out_gate", "taps", "docs"):
        fetches[name].wait()
    for r in range(length // 128):
        doc_rows[8 + r * 128 : 136 + r * 128, :] = jnp.broadcast_to(
            docs_v[r : r + 1, :].astype(F32), (128, 128)
        ).T
    for r in range(0, length, 256):
        product[8 + r : 264 + r, :] = buf_gate[0, r : r + 256, :256].astype(F32) * buf_gate[
            0, r : r + 256, 256:
        ].astype(F32)
    tap = [taps_v[k : k + 1, :].astype(F32) for k in range(3)]

    def convolve(r):
        here = doc_rows[8 + r : 264 + r, :]
        same = [doc_rows[6 + k + r : 262 + k + r, :] == here for k in range(2)]
        for h in (0, 128):
            total = tap[2][:, h : h + 128] * product[8 + r : 264 + r, h : h + 128]
            for k in range(2):
                term = tap[k][:, h : h + 128] * product[6 + k + r : 262 + k + r, h : h + 128]
                total = total + jnp.where(same[k], term, 0.0)
            gated[r : r + 256, h : h + 128] = (
                buf_gate[1, r : r + 256, h : h + 128].astype(F32) * total
            ).astype(BF16)

    for r in range(256, length, 256):
        convolve(r)
    cp.arrived("halo_c")
    cp.arrived("halo_g")
    cp.arrived("halo_d")
    product[:8, :] = (halo_c[...].astype(F32) * halo_g[...].astype(F32))[8:]
    halo_docs = jnp.broadcast_to(halo_d[7:8, :].astype(F32), (128, 128)).T
    doc_rows[:8, :] = jnp.where(sp == 0, -1.0, halo_docs[120:])
    convolve(0)

    for name, dev in (("r", right), ("l", left), ("a", across)):
        cp.start("mix_" + name, gated.at[strip(dev[1])], a2a.at[tp], dev)
    fetch("mix", gated.at[strip(tp)], a2a.at[tp])

    def share(kind, name, part, at):
        store = all_gate if kind == "gate" else all_up
        slot = 1 if name == "y" else 3
        cp.start(f"{kind}_o{part}_{name}", store.at[slot, at], store.at[slot + 1, at], other)

    def turn(kind, way, name, part, at):
        store = all_gate if kind == "gate" else all_up
        slot = 1 if name == "y" else 3
        cp.start(
            f"{kind}_{part}_{name}", store.at[slot, at], store.at[slot, at], right if way == "r" else left
        )

    before, after, opposite = strip((tp + 3) % 4), strip((tp + 1) % 4), strip((tp + 2) % 4)

    def early(k):
        return pl.ds(pl.multiple_of((k % 4) * rows, rows), rows - DIRECT)

    for name in ("y", "z"):
        cp.arrived("gate_" + name)
        turn("gate", "r", name, "r", mine)
        turn("gate", "l", name, "l", mine)
        share("gate", name, "m", mine)

    fetches["ids"].wait()
    fetches["route"].wait()
    experts = lax.broadcasted_iota(jnp.int32, (EXPERTS, rows), 0)
    hit = [ids_v[j : j + 1, :] == experts for j in range(2)]
    used = jnp.where(hit[0], 1.0, jnp.where(hit[1], 1.0, 0.0))
    earlier = lax.broadcasted_iota(jnp.int32, (rows, rows), 0) < lax.broadcasted_iota(jnp.int32, (rows, rows), 1)
    dispatch[...] = jnp.where(earlier, 1.0, 0.0).astype(BF16)
    rank = jnp.dot(used.astype(BF16), dispatch[...], preferred_element_type=F32)
    tables[0, :EXPERTS, :] = jnp.where(used > 0.0, rank, -1.0)
    tables[0, EXPERTS:, :] = jnp.where(hit[0], route_v[0:1, :], jnp.where(hit[1], route_v[1:2, :], 0.0))

    for name, dev, slot in (("y", far_y, 1), ("z", far_z, 2), ("d", far_d, 3)):
        cp.start("table_" + name, tables.at[0], tables.at[slot], dev)

    for name in ("mix", "proj0", "proj1", "res0", "res1", "gain"):
        fetches[name].wait()
    for name in ("r", "l", "a"):
        cp.arrived("mix_" + name)
    step = 512

    def project():
        squares = jnp.zeros((rows, 1), F32)
        for n in range(0, width, step):
            part = jnp.concatenate([rows_x[0, :, n : n + step], rows_x[1, :, n : n + step]], axis=0).astype(F32)
            for j in range(4):
                part = part + jnp.dot(
                    a2a[j],
                    buf_down[j // 2, (j % 2) * 256 : (j % 2 + 1) * 256, n : n + step],
                    preferred_element_type=F32,
                )
            hidden[:, n : n + step] = part
            squares = squares + jnp.sum(part * part, axis=1, keepdims=True)
        scale = lax.rsqrt(squares * (1.0 / width) + epsilon)
        for n in range(0, width, step):
            tok[0, :, n : n + step] = (hidden[:, n : n + step] * scale * gain_v[:, n : n + step]).astype(BF16)

    project()
    cp.start("tok_y", tok.at[0], tok.at[1], far_y)
    cp.start("tok_z", tok.at[0], tok.at[2], far_z)

    def matches(source, pair):
        slot = lax.broadcasted_iota(jnp.int32, (CAP, rows), 0).astype(F32)
        halves, weights = [], []
        for k in range(2):
            e = expert_of[2 * pair + k]
            same = tables[source, pl.ds(e, 1), :] == slot
            halves.append(jnp.where(same, 1.0, 0.0))
            weights.append(jnp.where(same, tables[source, pl.ds(EXPERTS + e, 1), :], 0.0))
        return jnp.concatenate(halves, axis=0), jnp.concatenate(weights, axis=0)

    source_of = [1, 2, 0, 3]

    def gather(i):
        source = source_of[i]
        for pair in range(4):
            dispatch[pair * 128 : (pair + 1) * 128, :] = matches(source, pair)[0].astype(BF16)
        for n in range(0, width, step):
            got = jnp.dot(dispatch[...], tok[source, :, n : n + step], preferred_element_type=F32).astype(BF16)
            for e in range(6):
                rows_x[e, i * CAP : (i + 1) * CAP, n : n + step] = got[e * CAP : (e + 1) * CAP]
            rows_di[i, :, n : n + step] = got[6 * CAP :]

    def weigh(i):
        for pair in range(4):
            combine[:, pair * 128 : (pair + 1) * 128] = matches(source_of[i], pair)[1].T.astype(BF16)

    def scatter(i, cols, store):
        for n in range(cols.start, cols.stop, step):
            total = jnp.dot(combine[:, :384], outs[i, :, n : n + step], preferred_element_type=F32)
            total = total + jnp.dot(combine[:, 384:], returned[i, :, n : n + step], preferred_element_type=F32)
            store(n, total)

    def load(e, slot):
        gate_from = w_gate if e == 0 else all_gate.at[e - 1]
        up_from = w_up if e == 0 else all_up.at[e - 1]
        down_from = w_down if e == 0 else all_down.at[e - 1]
        fetch(f"g{slot}", gate_from, buf_gate.at[slot], slot * 3)
        fetch(f"u{slot}", up_from, buf_up.at[slot], slot * 3 + 1)
        fetch(f"d{slot}", down_from, buf_down.at[slot], slot * 3 + 2)

    def loaded(slot):
        for kind in "gud":
            fetches[f"{kind}{slot}"].wait()

    def activate(slot, left_ref, high):
        for n in range(0, 512, 256):
            left_side = left_ref[...]
            gate_val = jnp.dot(left_side, buf_gate[slot, :, n : n + 256], preferred_element_type=F32)
            up_val = jnp.dot(left_side, buf_up[slot, :, n : n + 256], preferred_element_type=F32)
            act[:high, n : n + 256] = (gate_val / (1.0 + jnp.exp(-gate_val)) * up_val).astype(BF16)

    def local(e, slot, batch):
        activate(slot, rows_x.at[e, batch * 128 : (batch + 1) * 128], 128)
        for n in range(0, width, step):
            got = jnp.dot(act[...], buf_down[slot, :, n : n + step], preferred_element_type=F32).astype(BF16)
            for k in range(2):
                outs[2 * batch + k, e * CAP : (e + 1) * CAP, n : n + step] = got[k * CAP : (k + 1) * CAP]

    def distant(e, slot, i):
        at = slice((e % 2) * CAP, (e % 2 + 1) * CAP)
        activate(slot, rows_in.at[i, at], CAP)
        for n in range(0, width, step):
            outs_far[i, at, n : n + step] = jnp.dot(
                act[:CAP, :], buf_down[slot, :, n : n + step], preferred_element_type=F32
            ).astype(BF16)

    def ask(i):
        for k in range(2):
            at = slice(k * CAP, (k + 1) * CAP)
            by_y = k == 1 if i == 3 else i != 1
            cp.start(f"ask{i}{k}", rows_di.at[i, at], rows_in.at[i, at], near_y if by_y else near_z)

    def answer(e, i, order):
        at = slice((e % 2) * CAP, (e % 2 + 1) * CAP)
        for half in order:
            cols = A_COLS if half == "a" else B_COLS
            cp.start(
                f"ans{i}{e % 2}{half}",
                outs_far.at[i, at, cols],
                returned.at[i, at, cols],
                near_z if e < 4 else near_y,
            )

    def answered(i, half):
        for k in range(2):
            cp.arrived(f"ans{i}{k}{half}")

    gather(2)
    cp.arrived("up_y")
    turn("up", "r", "y", "r", mine)
    turn("up", "l", "y", "l", mine)
    share("up", "y", "m", mine)
    cp.arrived("gate_r_y")
    turn("gate", "r", "y", "f", early(tp + 3))
    share("gate", "y", "r", before)
    cp.arrived("up_z")
    turn("up", "r", "z", "r", mine)
    share("up", "z", "m", mine)
    cp.arrived("gate_l_y")
    share("gate", "y", "l", after)
    cp.arrived("gate_r_z")
    turn("gate", "r", "z", "f", before)
    share("gate", "z", "r", before)
    cp.arrived("up_d_z")
    share("up", "z", "d", late)
    cp.arrived("gate_l_z")
    share("gate", "z", "l", after)
    cp.arrived("up_l_y")
    turn("up", "l", "y", "f", after)
    turn("up", "l", "z", "l", mine)
    share("up", "y", "l", after)
    cp.arrived("up_r_y")
    share("up", "y", "r", before)
    for name in ("gate", "up", "down"):
        cp.arrived("own_" + name)
    load(0, 0)
    load(1, 1)
    cp.arrived("gate_f_y")
    share("gate", "y", "f", early(tp + 2))
    cp.arrived("gate_d_y")
    share("gate", "y", "d", late)
    cp.arrived("up_f_y")
    share("up", "y", "f", opposite)

    cp.arrived("tok_y")
    cp.start("tok_fy", tok.at[1, :HALF], tok.at[3, :HALF], far_z)
    cp.arrived("tok_z")
    cp.start("tok_fz", tok.at[2, HALF:], tok.at[3, HALF:], far_y)
    cp.arrived("table_y")
    gather(0)
    ask(0)
    cp.arrived("table_z")
    gather(1)
    ask(1)

    cp.arrived("down_y")
    cp.start("down_o_y", all_down.at[1], all_down.at[2], other)
    load(2, 2)
    cp.arrived("up_l_z")
    turn("up", "l", "z", "f", early(tp + 1))
    share("up", "z", "l", after)
    loaded(0)
    local(0, 0, 0)
    for kind, parts in (("gate", "mrlfd"), ("up", "mrlf")):
        for part in parts:
            cp.arrived(f"{kind}_o{part}_y")
    loaded(1)
    local(1, 1, 0)
    cp.arrived("up_r_z")
    share("up", "z", "r", before)
    cp.arrived("down_z")
    cp.start("down_o_z", all_down.at[3], all_down.at[4], other)
    loaded(2)
    local(2, 2, 0)
    cp.arrived("down_o_y")
    load(3, 0)
    cp.arrived("ask10")
    distant(2, 2, 1)
    answer(2, 1, "b")
    loaded(0)
    local(3, 0, 0)
    cp.arrived("gate_f_z")
    share("gate", "z", "f", opposite)
    cp.arrived("up_f_z")
    share("up", "z", "f", early(tp + 2))
    load(4, 1)
    cp.arrived("ask11")
    distant(3, 0, 1)
    answer(3, 1, "b")
    for kind, parts in (("gate", "mrlf"), ("up", "mrlfd")):
        for part in parts:
            cp.arrived(f"{kind}_o{part}_z")
    cp.arrived("down_o_z")
    load(5, 2)
    load(2, 0)
    cp.arrived("ask00")
    loaded(1)
    distant(4, 1, 0)
    answer(4, 0, "a")
    local(4, 1, 0)
    cp.arrived("ask01")
    loaded(2)
    distant(5, 2, 0)
    answer(5, 0, "a")
    local(5, 2, 0)

    def into(k, name=None, to=None, dev=None):
        def store(n, total):
            tok[k, :, n : n + step] = total.astype(BF16)
            if name is not None:
                r = n // step % 2
                cp.start(f"{name}{r}", tok.at[k, :, n : n + step], land.at[to, :, r * step : (r + 1) * step], dev)

        return store

    cp.sent("tok_fz")
    weigh(1)
    answered(1, "b")
    scatter(1, B_COLS, into(2, "pure_z", 1, far_z))
    cp.arrived("tok_fy")
    cp.arrived("tok_fz")
    cp.arrived("table_d")
    gather(3)
    ask(3)
    answer(4, 0, "b")
    answer(5, 0, "b")
    cp.sent("tok_fy")
    weigh(0)
    answered(0, "a")
    scatter(0, A_COLS, into(1, "pure_y", 0, far_y))

    local(5, 2, 1)
    local(4, 1, 1)
    loaded(0)
    local(2, 0, 1)
    cp.arrived("ask30")
    distant(2, 0, 3)
    answer(2, 3, "ba")
    load(3, 0)
    cp.arrived("ask31")
    distant(5, 2, 3)
    answer(5, 3, "ba")
    load(0, 2)
    answer(2, 1, "a")
    answer(3, 1, "a")
    ask(2)
    answered(0, "b")
    scatter(0, B_COLS, into(1))
    loaded(0)
    local(3, 0, 1)
    load(1, 0)
    loaded(2)
    local(0, 2, 1)
    load(5, 2)
    weigh(3)
    loaded(0)
    local(1, 0, 1)
    answered(3, "b")
    scatter(3, B_COLS, into(3, "diag_z", 3, far_z))
    answered(3, "a")
    scatter(3, A_COLS, into(3, "diag_y", 2, far_y))
    weigh(1)
    answered(1, "a")
    scatter(1, A_COLS, into(2))
    cp.arrived("ask20")
    distant(4, 1, 2)
    answer(4, 2, "ab")
    cp.arrived("ask21")
    loaded(2)
    distant(5, 2, 2)
    answer(5, 2, "ab")

    def onto_hidden(n, total):
        hidden[:, n : n + step] = hidden[:, n : n + step] + total

    weigh(2)
    answered(2, "a")
    answered(2, "b")
    scatter(2, A_COLS, onto_hidden)
    scatter(2, B_COLS, onto_hidden)
    for r in range(2):
        cp.arrived(f"pure_z{r}")
        cp.arrived(f"pure_y{r}")
    hidden[:, A_COLS] = hidden[:, A_COLS] + land[0].astype(F32)
    hidden[:, B_COLS] = hidden[:, B_COLS] + land[1].astype(F32)
    fetch("hidden", hidden, hidden_out)

    for r in range(2):
        at, to_a, to_b = (slice(k + r * step, k + (r + 1) * step) for k in (0, 0, 1024))
        cp.arrived(f"diag_z{r}")
        tok[1, :, to_b] = (tok[1, :, to_b].astype(F32) + land[3, :, at].astype(F32)).astype(BF16)
        cp.start(f"fwd_y{r}", tok.at[1, :, to_b], far_out.at[:, to_b], far_y)
        cp.arrived(f"diag_y{r}")
        tok[2, :, to_a] = (tok[2, :, to_a].astype(F32) + land[2, :, at].astype(F32)).astype(BF16)
        cp.start(f"fwd_z{r}", tok.at[2, :, to_a], far_out.at[:, to_a], far_z)
    fetches["hidden"].wait()
    for name in [name for name in cp.unsent if not name.startswith("fwd")]:
        cp.sent(name)
    for r in range(2):
        cp.arrived(f"fwd_z{r}")
        cp.arrived(f"fwd_y{r}")
    cp.finish()


def layer(*operands):
    residual, w_gate = operands[0], operands[10]
    rows, width = residual.shape
    hid = w_gate.shape[1]
    length, channels = operands[1].shape
    any_spec = pl.BlockSpec(memory_space=pl.ANY)
    shapes = (
        jax.ShapeDtypeStruct((rows, width), F32),
        jax.ShapeDtypeStruct((rows, width), BF16),
        jax.ShapeDtypeStruct((5, width, hid), BF16),
        jax.ShapeDtypeStruct((5, width, hid), BF16),
        jax.ShapeDtypeStruct((5, hid, width), BF16),
    )
    hidden, far = pl.pallas_call(
        layer_kernel,
        out_shape=shapes,
        in_specs=[any_spec] * len(operands),
        out_specs=(any_spec,) * 5,
        scratch_shapes=[
            pltpu.VMEM((3, channels), BF16),
            pltpu.VMEM((length // 128, 128), jnp.int32),
            pltpu.VMEM((2, rows), jnp.int32),
            pltpu.VMEM((2, rows), F32),
            pltpu.VMEM((16, channels), BF16),
            pltpu.VMEM((16, channels), BF16),
            pltpu.VMEM((8, 128), jnp.int32),
            pltpu.VMEM((length + 8, channels), F32),
            pltpu.VMEM((length + 8, 128), F32),
            pltpu.VMEM((length, channels), BF16),
            pltpu.VMEM((4, rows, channels), BF16),
            pltpu.VMEM((1, width), F32),
            pltpu.VMEM((rows, width), F32),
            pltpu.VMEM((4, rows, width), BF16),
            pltpu.VMEM((4, 2 * EXPERTS, rows), F32),
            pltpu.VMEM((512, rows), BF16),
            pltpu.VMEM((rows, 512), BF16),
            pltpu.VMEM((6, 256, width), BF16),
            pltpu.VMEM((4, 128, width), BF16),
            pltpu.VMEM((4, 128, width), BF16),
            pltpu.VMEM((128, hid), BF16),
            pltpu.VMEM((4, 384, width), BF16),
            pltpu.VMEM((4, 128, width), BF16),
            pltpu.VMEM((4, 128, width), BF16),
            pltpu.VMEM((4, rows, width // 2), BF16),
            pltpu.VMEM((3, width, hid), BF16),
            pltpu.VMEM((3, width, hid), BF16),
            pltpu.VMEM((3, hid, width), BF16),
            pltpu.SemaphoreType.DMA((COPIES,)),
            pltpu.SemaphoreType.DMA((COPIES,)),
            pltpu.SemaphoreType.DMA((LOCALS + 16,)),
        ],
        compiler_params=pltpu.CompilerParams(
            collective_id=0, has_side_effects=True, vmem_limit_bytes=67043328
        ),
        name="layer",
    )(*operands)[:2]
    return (hidden + far.astype(F32)).astype(BF16)


def per_device(
    residual_in,
    conv_input,
    input_gate,
    output_gate,
    conv_taps,
    doc_ids,
    proj_weight,
    norm_gain,
    expert_ids,
    expert_weight,
    w_gate,
    w_up,
    w_down,
):
    return layer(
        residual_in,
        conv_input,
        input_gate,
        output_gate,
        conv_taps,
        doc_ids.reshape(-1, 128),
        proj_weight,
        norm_gain[None, :],
        expert_ids.T,
        expert_weight.T,
        w_gate[0],
        w_up[0],
        w_down[0],
    )


def solution(mesh):
    return jax.shard_map(
        per_device,
        mesh=mesh,
        in_specs=(
            P(("sp", "tp"), None),
            P("sp", "tp"),
            P("sp", "tp"),
            P("sp", "tp"),
            P(None, "tp"),
            P("sp"),
            P(),
            P(),
            P(("sp", "tp"), None),
            P(("sp", "tp"), None),
            P("sp", None, None),
            P("sp", None, None),
            P("sp", None, None),
        ),
        out_specs=P(("sp", "tp"), None),
        check_vma=False,
    )
```

```python
import jax
import jax.numpy as jnp
from jax import lax
from jax.experimental import pallas as pl
from jax.experimental.pallas import tpu as pltpu
from jax.sharding import PartitionSpec as P

EXPERTS = 32
CAP = 64
epsilon = 1e-06
F32 = jnp.float32
BF16 = jnp.bfloat16
MESH = pl.DeviceIdType.MESH
HALF = 256
DIRECT = 128


class Copies:
    def __init__(self, send_sem, recv_sem):
        self.send_sem, self.recv_sem = send_sem, recv_sem
        self.made = {}
        self.unsent = []

    def start(self, name, src, dst, device):
        i = len(self.made)
        copy = pltpu.make_async_remote_copy(
            src_ref=src,
            dst_ref=dst,
            send_sem=self.send_sem.at[i],
            recv_sem=self.recv_sem.at[i],
            device_id=device,
            device_id_type=MESH,
        )
        self.made[name] = copy
        self.unsent.append(name)
        copy.start()

    def arrived(self, name):
        self.made[name].wait_recv()

    def sent(self, name):
        self.made[name].wait_send()
        self.unsent.remove(name)

    def finish(self):
        for name in list(self.unsent):
            self.sent(name)


COPIES = 112
LOCALS = 64
A_COLS, B_COLS = slice(0, 1024), slice(1024, 2048)


def layer_kernel(
    residual,
    conv_input,
    input_gate,
    output_gate,
    taps,
    docs,
    proj,
    gain,
    ids,
    route_weight,
    w_gate,
    w_up,
    w_down,
    hidden_out,
    far_out,
    all_gate,
    all_up,
    all_down,
    taps_v,
    docs_v,
    ids_v,
    route_v,
    halo_c,
    halo_g,
    halo_d,
    product,
    doc_rows,
    gated,
    a2a,
    gain_v,
    hidden,
    tok,
    tables,
    dispatch,
    combine,
    rows_x,
    rows_di,
    rows_in,
    act,
    outs,
    outs_far,
    returned,
    land,
    buf_gate,
    buf_up,
    buf_down,
    send_sem,
    recv_sem,
    local_sem,
):
    sp, tp = lax.axis_index("sp"), lax.axis_index("tp")
    z, y, c = sp // 8, (sp // 2) % 4, sp % 2
    rows, width = tok.shape[1], tok.shape[2]
    length = gated.shape[0]

    def place(yy, zz, cc):
        return zz * 8 + yy * 2 + cc

    y_in, z_in = y + 1 - 2 * (y % 2), z + 1 - 2 * (z % 2)
    near_y, near_z = (place(y_in, z, c), tp), (place(y, z_in, c), tp)
    far_y, far_z = (place(3 - y, z, c), tp), (place(y, 3 - z, c), tp)
    far_d = (place(3 - y, 3 - z, c), tp)
    other = (place(y, z, 1 - c), tp)
    right, left = (sp, (tp + 1) % 4), (sp, (tp + 3) % 4)
    across = (sp, (tp + 2) % 4)
    ahead, behind = ((sp + 1) % 32, tp), ((sp + 31) % 32, tp)
    chips = [(y, z), (y_in, z), (y, z_in), (y_in, z_in)]
    expert_of = [place(yy, zz, cc) for yy, zz in chips for cc in (c, 1 - c)]

    barrier = pltpu.get_barrier_semaphore()
    partners = [near_y, near_z, far_y, far_z, far_d, other, right, left, across, ahead, behind]
    for partner in partners:
        pl.semaphore_signal(barrier, inc=1, device_id=partner, device_id_type=MESH)

    cp = Copies(send_sem, recv_sem)
    fetches, pending = {}, {}

    def fetch(name, src, dst, i=None):
        i = 9 + len(fetches) if i is None else i
        fetches[name] = pltpu.make_async_copy(src, dst, local_sem.at[i])
        fetches[name].start()

    def strip(k):
        return pl.ds(pl.multiple_of(k * rows, rows), rows)

    conv_v, in_gate_v = buf_gate.at[0, :, :256], buf_gate.at[0, :, 256:]
    out_gate_v = buf_gate.at[1, :, :256]
    fetch("conv", conv_input, conv_v)
    fetch("in_gate", input_gate, in_gate_v)
    fetch("out_gate", output_gate, out_gate_v)
    fetch("taps", taps, taps_v)
    fetch("docs", docs, docs_v)
    fetch("ids", ids, ids_v)
    fetch("route", route_weight, route_v)
    fetch("gain", gain, gain_v)
    fetch("proj0", proj.at[:512], buf_down.at[0])
    fetch("proj1", proj.at[512:], buf_down.at[1])
    fetch("res0", residual.at[:256], rows_x.at[0])
    fetch("res1", residual.at[256:], rows_x.at[1])
    pl.semaphore_wait(barrier, len(partners))

    cp.start("halo_c", conv_input.at[length - 16 :], halo_c, ahead)
    cp.start("halo_g", input_gate.at[length - 16 :], halo_g, ahead)
    cp.start("halo_d", docs.at[8:], halo_d, ahead)
    mine = strip(tp)
    near = (("y", near_y, 1), ("z", near_z, 3))
    for name, dev, slot in near:
        cp.start("gate_" + name, w_gate.at[mine], all_gate.at[slot, mine], dev)
    for name, dev, slot in near:
        cp.start("up_" + name, w_up.at[mine], all_up.at[slot, mine], dev)
    late = pl.ds(pl.multiple_of(((tp + 2) % 4) * rows + rows - DIRECT, DIRECT), DIRECT)
    cp.start("gate_d_y", w_gate.at[late], all_gate.at[1, late], near_y)
    cp.start("up_d_z", w_up.at[late], all_up.at[3, late], near_z)
    for name, dev, slot in near:
        cp.start("down_" + name, w_down, all_down.at[slot], dev)
    cp.start("own_gate", w_gate, all_gate.at[0], other)
    cp.start("own_up", w_up, all_up.at[0], other)
    cp.start("own_down", w_down, all_down.at[0], other)

    for name in ("conv", "in_gate", "out_gate", "taps", "docs"):
        fetches[name].wait()
    for r in range(length // 128):
        doc_rows[8 + r * 128 : 136 + r * 128, :] = jnp.broadcast_to(
            docs_v[r : r + 1, :].astype(F32), (128, 128)
        ).T
    for r in range(0, length, 256):
        product[8 + r : 264 + r, :] = buf_gate[0, r : r + 256, :256].astype(F32) * buf_gate[
            0, r : r + 256, 256:
        ].astype(F32)
    tap = [taps_v[k : k + 1, :].astype(F32) for k in range(3)]

    def convolve(r):
        here = doc_rows[8 + r : 264 + r, :]
        same = [doc_rows[6 + k + r : 262 + k + r, :] == here for k in range(2)]
        for h in (0, 128):
            total = tap[2][:, h : h + 128] * product[8 + r : 264 + r, h : h + 128]
            for k in range(2):
                term = tap[k][:, h : h + 128] * product[6 + k + r : 262 + k + r, h : h + 128]
                total = total + jnp.where(same[k], term, 0.0)
            gated[r : r + 256, h : h + 128] = (
                buf_gate[1, r : r + 256, h : h + 128].astype(F32) * total
            ).astype(BF16)

    for r in range(256, length, 256):
        convolve(r)
    cp.arrived("halo_c")
    cp.arrived("halo_g")
    cp.arrived("halo_d")
    product[:8, :] = (halo_c[...].astype(F32) * halo_g[...].astype(F32))[8:]
    halo_docs = jnp.broadcast_to(halo_d[7:8, :].astype(F32), (128, 128)).T
    doc_rows[:8, :] = jnp.where(sp == 0, -1.0, halo_docs[120:])
    convolve(0)

    for name, dev in (("r", right), ("l", left), ("a", across)):
        cp.start("mix_" + name, gated.at[strip(dev[1])], a2a.at[tp], dev)
    fetch("mix", gated.at[strip(tp)], a2a.at[tp])

    def share(kind, name, part, at):
        store = all_gate if kind == "gate" else all_up
        slot = 1 if name == "y" else 3
        cp.start(f"{kind}_o{part}_{name}", store.at[slot, at], store.at[slot + 1, at], other)

    def turn(kind, way, name, part, at):
        store = all_gate if kind == "gate" else all_up
        slot = 1 if name == "y" else 3
        cp.start(
            f"{kind}_{part}_{name}", store.at[slot, at], store.at[slot, at], right if way == "r" else left
        )

    before, after, opposite = strip((tp + 3) % 4), strip((tp + 1) % 4), strip((tp + 2) % 4)

    def early(k):
        return pl.ds(pl.multiple_of((k % 4) * rows, rows), rows - DIRECT)

    for name in ("y", "z"):
        cp.arrived("gate_" + name)
        turn("gate", "r", name, "r", mine)
        turn("gate", "l", name, "l", mine)
        share("gate", name, "m", mine)

    fetches["ids"].wait()
    fetches["route"].wait()
    experts = lax.broadcasted_iota(jnp.int32, (EXPERTS, rows), 0)
    hit = [ids_v[j : j + 1, :] == experts for j in range(2)]
    used = jnp.where(hit[0], 1.0, jnp.where(hit[1], 1.0, 0.0))
    earlier = lax.broadcasted_iota(jnp.int32, (rows, rows), 0) < lax.broadcasted_iota(jnp.int32, (rows, rows), 1)
    dispatch[...] = jnp.where(earlier, 1.0, 0.0).astype(BF16)
    rank = jnp.dot(used.astype(BF16), dispatch[...], preferred_element_type=F32)
    tables[0, :EXPERTS, :] = jnp.where(used > 0.0, rank, -1.0)
    tables[0, EXPERTS:, :] = jnp.where(hit[0], route_v[0:1, :], jnp.where(hit[1], route_v[1:2, :], 0.0))

    for name, dev, slot in (("y", far_y, 1), ("z", far_z, 2), ("d", far_d, 3)):
        cp.start("table_" + name, tables.at[0], tables.at[slot], dev)

    for name in ("mix", "proj0", "proj1", "res0", "res1", "gain"):
        fetches[name].wait()
    for name in ("r", "l", "a"):
        cp.arrived("mix_" + name)
    step = 512

    def project():
        squares = jnp.zeros((rows, 1), F32)
        for n in range(0, width, step):
            part = jnp.concatenate([rows_x[0, :, n : n + step], rows_x[1, :, n : n + step]], axis=0).astype(F32)
            for j in range(4):
                part = part + jnp.dot(
                    a2a[j],
                    buf_down[j // 2, (j % 2) * 256 : (j % 2 + 1) * 256, n : n + step],
                    preferred_element_type=F32,
                )
            hidden[:, n : n + step] = part
            squares = squares + jnp.sum(part * part, axis=1, keepdims=True)
        scale = lax.rsqrt(squares * (1.0 / width) + epsilon)
        for n in range(0, width, step):
            tok[0, :, n : n + step] = (hidden[:, n : n + step] * scale * gain_v[:, n : n + step]).astype(BF16)

    project()
    cp.start("tok_y", tok.at[0], tok.at[1], far_y)
    cp.start("tok_z", tok.at[0], tok.at[2], far_z)

    def matches(source, pair):
        slot = lax.broadcasted_iota(jnp.int32, (CAP, rows), 0).astype(F32)
        halves, weights = [], []
        for k in range(2):
            e = expert_of[2 * pair + k]
            same = tables[source, pl.ds(e, 1), :] == slot
            halves.append(jnp.where(same, 1.0, 0.0))
            weights.append(jnp.where(same, tables[source, pl.ds(EXPERTS + e, 1), :], 0.0))
        return jnp.concatenate(halves, axis=0), jnp.concatenate(weights, axis=0)

    source_of = [1, 2, 0, 3]

    def gather(i):
        source = source_of[i]
        for pair in range(4):
            dispatch[pair * 128 : (pair + 1) * 128, :] = matches(source, pair)[0].astype(BF16)
        for n in range(0, width, step):
            got = jnp.dot(dispatch[...], tok[source, :, n : n + step], preferred_element_type=F32).astype(BF16)
            for e in range(6):
                rows_x[e, i * CAP : (i + 1) * CAP, n : n + step] = got[e * CAP : (e + 1) * CAP]
            rows_di[i, :, n : n + step] = got[6 * CAP :]

    def weigh(i):
        for pair in range(4):
            combine[:, pair * 128 : (pair + 1) * 128] = matches(source_of[i], pair)[1].T.astype(BF16)

    def scatter(i, cols, store):
        for n in range(cols.start, cols.stop, step):
            total = jnp.dot(combine[:, :384], outs[i, :, n : n + step], preferred_element_type=F32)
            total = total + jnp.dot(combine[:, 384:], returned[i, :, n : n + step], preferred_element_type=F32)
            store(n, total)

    def load(e, slot):
        gate_from = w_gate if e == 0 else all_gate.at[e - 1]
        up_from = w_up if e == 0 else all_up.at[e - 1]
        down_from = w_down if e == 0 else all_down.at[e - 1]
        fetch(f"g{slot}", gate_from, buf_gate.at[slot], slot * 3)
        fetch(f"u{slot}", up_from, buf_up.at[slot], slot * 3 + 1)
        fetch(f"d{slot}", down_from, buf_down.at[slot], slot * 3 + 2)
        pending[slot] = [f"{kind}{slot}" for kind in "gud"]

    def load_early(e, slot):
        names = []
        for k, at in enumerate((mine, before, after)):
            fetch(f"g{e}{k}", all_gate.at[e - 1, at], buf_gate.at[slot, at])
            fetch(f"u{e}{k}", all_up.at[e - 1, at], buf_up.at[slot, at])
            names += [f"g{e}{k}", f"u{e}{k}"]
        fetch(f"u{e}d", all_up.at[e - 1, late], buf_up.at[slot, late])
        fetch(f"d{e}d", all_down.at[e - 1], buf_down.at[slot])
        pending[slot] = names + [f"u{e}d", f"d{e}d"]

    def load_late(e, slot):
        fetch(f"g{e}f", all_gate.at[e - 1, opposite], buf_gate.at[slot, opposite])
        fetch(f"u{e}f", all_up.at[e - 1, early(tp + 2)], buf_up.at[slot, early(tp + 2)])
        pending[slot] += [f"g{e}f", f"u{e}f"]

    def loaded(slot):
        for name in pending[slot]:
            fetches[name].wait()

    def activate(slot, left_ref, high):
        for n in range(0, 512, 256):
            left_side = left_ref[...]
            gate_val = jnp.dot(left_side, buf_gate[slot, :, n : n + 256], preferred_element_type=F32)
            up_val = jnp.dot(left_side, buf_up[slot, :, n : n + 256], preferred_element_type=F32)
            act[:high, n : n + 256] = (gate_val / (1.0 + jnp.exp(-gate_val)) * up_val).astype(BF16)

    def local(e, slot, batch):
        activate(slot, rows_x.at[e, batch * 128 : (batch + 1) * 128], 128)
        for n in range(0, width, step):
            got = jnp.dot(act[...], buf_down[slot, :, n : n + step], preferred_element_type=F32).astype(BF16)
            for k in range(2):
                outs[2 * batch + k, e * CAP : (e + 1) * CAP, n : n + step] = got[k * CAP : (k + 1) * CAP]

    def distant(e, slot, i):
        at = slice((e % 2) * CAP, (e % 2 + 1) * CAP)
        activate(slot, rows_in.at[i, at], CAP)
        for n in range(0, width, step):
            outs_far[i, at, n : n + step] = jnp.dot(
                act[:CAP, :], buf_down[slot, :, n : n + step], preferred_element_type=F32
            ).astype(BF16)

    def ask(i):
        for k in range(2):
            at = slice(k * CAP, (k + 1) * CAP)
            by_y = k == 1 if i == 3 else i != 1
            cp.start(f"ask{i}{k}", rows_di.at[i, at], rows_in.at[i, at], near_y if by_y else near_z)

    def answer(e, i, order):
        at = slice((e % 2) * CAP, (e % 2 + 1) * CAP)
        for half in order:
            cols = A_COLS if half == "a" else B_COLS
            cp.start(
                f"ans{i}{e % 2}{half}",
                outs_far.at[i, at, cols],
                returned.at[i, at, cols],
                near_z if e < 4 else near_y,
            )

    def answered(i, half):
        for k in range(2):
            cp.arrived(f"ans{i}{k}{half}")

    gather(2)
    cp.arrived("up_y")
    turn("up", "r", "y", "r", mine)
    turn("up", "l", "y", "l", mine)
    share("up", "y", "m", mine)
    cp.arrived("gate_r_y")
    turn("gate", "r", "y", "f", early(tp + 3))
    share("gate", "y", "r", before)
    cp.arrived("up_z")
    turn("up", "r", "z", "r", mine)
    share("up", "z", "m", mine)
    cp.arrived("gate_l_y")
    share("gate", "y", "l", after)
    cp.arrived("gate_r_z")
    turn("gate", "r", "z", "f", before)
    share("gate", "z", "r", before)
    cp.arrived("up_d_z")
    share("up", "z", "d", late)
    cp.arrived("gate_l_z")
    share("gate", "z", "l", after)
    cp.arrived("up_l_y")
    turn("up", "l", "y", "f", after)
    turn("up", "l", "z", "l", mine)
    share("up", "y", "l", after)
    cp.arrived("up_r_y")
    share("up", "y", "r", before)
    for name in ("gate", "up", "down"):
        cp.arrived("own_" + name)
    load(0, 0)
    load(1, 1)
    cp.arrived("gate_f_y")
    share("gate", "y", "f", early(tp + 2))
    cp.arrived("gate_d_y")
    share("gate", "y", "d", late)
    cp.arrived("up_f_y")
    share("up", "y", "f", opposite)

    cp.arrived("tok_y")
    cp.start("tok_fy", tok.at[1, :HALF], tok.at[3, :HALF], far_z)
    cp.arrived("tok_z")
    cp.start("tok_fz", tok.at[2, HALF:], tok.at[3, HALF:], far_y)
    cp.arrived("table_y")
    gather(0)
    ask(0)
    cp.arrived("table_z")
    gather(1)
    ask(1)

    cp.arrived("down_y")
    cp.start("down_o_y", all_down.at[1], all_down.at[2], other)
    load(2, 2)
    cp.arrived("up_l_z")
    turn("up", "l", "z", "f", early(tp + 1))
    share("up", "z", "l", after)
    loaded(0)
    local(0, 0, 0)
    for kind, parts in (("gate", "mrlfd"), ("up", "mrlf")):
        for part in parts:
            cp.arrived(f"{kind}_o{part}_y")
    loaded(1)
    local(1, 1, 0)
    cp.arrived("up_r_z")
    share("up", "z", "r", before)
    cp.arrived("down_z")
    cp.start("down_o_z", all_down.at[3], all_down.at[4], other)
    load_early(4, 1)
    loaded(2)
    local(2, 2, 0)
    cp.arrived("down_o_y")
    load(3, 0)
    cp.arrived("ask10")
    distant(2, 2, 1)
    answer(2, 1, "b")
    loaded(0)
    local(3, 0, 0)
    for part in ("gate_om", "gate_or", "gate_ol", "up_om", "up_or", "up_ol", "up_od", "down_o"):
        cp.arrived(part + "_z")
    load_early(5, 2)
    cp.arrived("gate_f_z")
    share("gate", "z", "f", opposite)
    cp.arrived("up_f_z")
    share("up", "z", "f", early(tp + 2))
    load_late(4, 1)
    cp.arrived("ask11")
    distant(3, 0, 1)
    answer(3, 1, "b")
    cp.arrived("ask00")
    loaded(1)
    distant(4, 1, 0)
    answer(4, 0, "a")
    cp.arrived("gate_of_z")
    cp.arrived("up_of_z")
    load_late(5, 2)
    load(2, 0)
    local(4, 1, 0)
    cp.arrived("ask01")
    loaded(2)
    distant(5, 2, 0)
    answer(5, 0, "a")
    local(5, 2, 0)

    def into(k, name=None, to=None, dev=None):
        def store(n, total):
            tok[k, :, n : n + step] = total.astype(BF16)
            if name is not None:
                r = n // step % 2
                cp.start(f"{name}{r}", tok.at[k, :, n : n + step], land.at[to, :, r * step : (r + 1) * step], dev)

        return store

    cp.sent("tok_fz")
    weigh(1)
    answered(1, "b")
    scatter(1, B_COLS, into(2, "pure_z", 1, far_z))
    cp.arrived("tok_fy")
    cp.arrived("tok_fz")
    cp.arrived("table_d")
    gather(3)
    ask(3)
    answer(4, 0, "b")
    answer(5, 0, "b")
    cp.sent("tok_fy")
    weigh(0)
    answered(0, "a")
    scatter(0, A_COLS, into(1, "pure_y", 0, far_y))

    local(5, 2, 1)
    local(4, 1, 1)
    loaded(0)
    local(2, 0, 1)
    cp.arrived("ask30")
    distant(2, 0, 3)
    answer(2, 3, "ba")
    load(3, 0)
    cp.arrived("ask31")
    distant(5, 2, 3)
    answer(5, 3, "ba")
    load(0, 2)
    answer(2, 1, "a")
    answer(3, 1, "a")
    ask(2)
    answered(0, "b")
    scatter(0, B_COLS, into(1))
    loaded(0)
    local(3, 0, 1)
    load(1, 0)
    loaded(2)
    local(0, 2, 1)
    load(5, 2)
    weigh(3)
    loaded(0)
    local(1, 0, 1)
    answered(3, "b")
    scatter(3, B_COLS, into(3, "diag_z", 3, far_z))
    answered(3, "a")
    scatter(3, A_COLS, into(3, "diag_y", 2, far_y))
    weigh(1)
    answered(1, "a")
    scatter(1, A_COLS, into(2))
    cp.arrived("ask20")
    distant(4, 1, 2)
    answer(4, 2, "ab")
    cp.arrived("ask21")
    loaded(2)
    distant(5, 2, 2)
    answer(5, 2, "ab")

    def onto_hidden(n, total):
        hidden[:, n : n + step] = hidden[:, n : n + step] + total

    weigh(2)
    answered(2, "a")
    answered(2, "b")
    scatter(2, A_COLS, onto_hidden)
    scatter(2, B_COLS, onto_hidden)
    for r in range(2):
        cp.arrived(f"pure_z{r}")
        cp.arrived(f"pure_y{r}")
    hidden[:, A_COLS] = hidden[:, A_COLS] + land[0].astype(F32)
    hidden[:, B_COLS] = hidden[:, B_COLS] + land[1].astype(F32)
    fetch("hidden", hidden, hidden_out)

    for r in range(2):
        at, to_a, to_b = (slice(k + r * step, k + (r + 1) * step) for k in (0, 0, 1024))
        cp.arrived(f"diag_z{r}")
        tok[1, :, to_b] = (tok[1, :, to_b].astype(F32) + land[3, :, at].astype(F32)).astype(BF16)
        cp.start(f"fwd_y{r}", tok.at[1, :, to_b], far_out.at[:, to_b], far_y)
        cp.arrived(f"diag_y{r}")
        tok[2, :, to_a] = (tok[2, :, to_a].astype(F32) + land[2, :, at].astype(F32)).astype(BF16)
        cp.start(f"fwd_z{r}", tok.at[2, :, to_a], far_out.at[:, to_a], far_z)
    fetches["hidden"].wait()
    for name in [name for name in cp.unsent if not name.startswith("fwd")]:
        cp.sent(name)
    for r in range(2):
        cp.arrived(f"fwd_z{r}")
        cp.arrived(f"fwd_y{r}")
    cp.finish()


def layer(*operands):
    residual, w_gate = operands[0], operands[10]
    rows, width = residual.shape
    hid = w_gate.shape[1]
    length, channels = operands[1].shape
    any_spec = pl.BlockSpec(memory_space=pl.ANY)
    shapes = (
        jax.ShapeDtypeStruct((rows, width), F32),
        jax.ShapeDtypeStruct((rows, width), BF16),
        jax.ShapeDtypeStruct((5, width, hid), BF16),
        jax.ShapeDtypeStruct((5, width, hid), BF16),
        jax.ShapeDtypeStruct((5, hid, width), BF16),
    )
    hidden, far = pl.pallas_call(
        layer_kernel,
        out_shape=shapes,
        in_specs=[any_spec] * len(operands),
        out_specs=(any_spec,) * 5,
        scratch_shapes=[
            pltpu.VMEM((3, channels), BF16),
            pltpu.VMEM((length // 128, 128), jnp.int32),
            pltpu.VMEM((2, rows), jnp.int32),
            pltpu.VMEM((2, rows), F32),
            pltpu.VMEM((16, channels), BF16),
            pltpu.VMEM((16, channels), BF16),
            pltpu.VMEM((8, 128), jnp.int32),
            pltpu.VMEM((length + 8, channels), F32),
            pltpu.VMEM((length + 8, 128), F32),
            pltpu.VMEM((length, channels), BF16),
            pltpu.VMEM((4, rows, channels), BF16),
            pltpu.VMEM((1, width), F32),
            pltpu.VMEM((rows, width), F32),
            pltpu.VMEM((4, rows, width), BF16),
            pltpu.VMEM((4, 2 * EXPERTS, rows), F32),
            pltpu.VMEM((512, rows), BF16),
            pltpu.VMEM((rows, 512), BF16),
            pltpu.VMEM((6, 256, width), BF16),
            pltpu.VMEM((4, 128, width), BF16),
            pltpu.VMEM((4, 128, width), BF16),
            pltpu.VMEM((128, hid), BF16),
            pltpu.VMEM((4, 384, width), BF16),
            pltpu.VMEM((4, 128, width), BF16),
            pltpu.VMEM((4, 128, width), BF16),
            pltpu.VMEM((4, rows, width // 2), BF16),
            pltpu.VMEM((3, width, hid), BF16),
            pltpu.VMEM((3, width, hid), BF16),
            pltpu.VMEM((3, hid, width), BF16),
            pltpu.SemaphoreType.DMA((COPIES,)),
            pltpu.SemaphoreType.DMA((COPIES,)),
            pltpu.SemaphoreType.DMA((LOCALS,)),
        ],
        compiler_params=pltpu.CompilerParams(
            collective_id=0, has_side_effects=True, vmem_limit_bytes=67043328
        ),
        name="layer",
    )(*operands)[:2]
    return (hidden + far.astype(F32)).astype(BF16)


def per_device(
    residual_in,
    conv_input,
    input_gate,
    output_gate,
    conv_taps,
    doc_ids,
    proj_weight,
    norm_gain,
    expert_ids,
    expert_weight,
    w_gate,
    w_up,
    w_down,
):
    return layer(
        residual_in,
        conv_input,
        input_gate,
        output_gate,
        conv_taps,
        doc_ids.reshape(-1, 128),
        proj_weight,
        norm_gain[None, :],
        expert_ids.T,
        expert_weight.T,
        w_gate[0],
        w_up[0],
        w_down[0],
    )


def solution(mesh):
    return jax.shard_map(
        per_device,
        mesh=mesh,
        in_specs=(
            P(("sp", "tp"), None),
            P("sp", "tp"),
            P("sp", "tp"),
            P("sp", "tp"),
            P(None, "tp"),
            P("sp"),
            P(),
            P(),
            P(("sp", "tp"), None),
            P(("sp", "tp"), None),
            P("sp", None, None),
            P("sp", None, None),
            P("sp", None, None),
        ),
        out_specs=P(("sp", "tp"), None),
        check_vma=False,
    )
```

```python
import jax
import jax.numpy as jnp
from jax import lax
from jax.experimental import pallas as pl
from jax.experimental.pallas import tpu as pltpu
from jax.sharding import PartitionSpec as P

EXPERTS = 32
CAP = 64
epsilon = 1e-06
F32 = jnp.float32
BF16 = jnp.bfloat16
MESH = pl.DeviceIdType.MESH
HALF = 256
DIRECT = 128


class Copies:
    def __init__(self, send_sem, recv_sem):
        self.send_sem, self.recv_sem = send_sem, recv_sem
        self.made = {}
        self.unsent = []

    def start(self, name, src, dst, device):
        i = len(self.made)
        copy = pltpu.make_async_remote_copy(
            src_ref=src,
            dst_ref=dst,
            send_sem=self.send_sem.at[i],
            recv_sem=self.recv_sem.at[i],
            device_id=device,
            device_id_type=MESH,
        )
        self.made[name] = copy
        self.unsent.append(name)
        copy.start()

    def arrived(self, name):
        self.made[name].wait_recv()

    def sent(self, name):
        self.made[name].wait_send()
        self.unsent.remove(name)

    def finish(self):
        for name in list(self.unsent):
            self.sent(name)


COPIES = 112
LOCALS = 24
A_COLS, B_COLS = slice(0, 1024), slice(1024, 2048)


def layer_kernel(
    residual,
    conv_input,
    input_gate,
    output_gate,
    taps,
    docs,
    proj,
    gain,
    ids,
    route_weight,
    w_gate,
    w_up,
    w_down,
    hidden_out,
    far_out,
    all_gate,
    all_up,
    all_down,
    taps_v,
    docs_v,
    ids_v,
    route_v,
    halo_c,
    halo_g,
    halo_d,
    product,
    doc_rows,
    gated,
    a2a,
    gain_v,
    hidden,
    tok,
    tables,
    dispatch,
    combine,
    rows_x,
    rows_di,
    rows_in,
    act,
    outs,
    outs_far,
    returned,
    land,
    buf_gate,
    buf_up,
    buf_down,
    send_sem,
    recv_sem,
    local_sem,
):
    sp, tp = lax.axis_index("sp"), lax.axis_index("tp")
    z, y, c = sp // 8, (sp // 2) % 4, sp % 2
    rows, width = tok.shape[1], tok.shape[2]
    length = gated.shape[0]

    def place(yy, zz, cc):
        return zz * 8 + yy * 2 + cc

    y_in, z_in = y + 1 - 2 * (y % 2), z + 1 - 2 * (z % 2)
    near_y, near_z = (place(y_in, z, c), tp), (place(y, z_in, c), tp)
    far_y, far_z = (place(3 - y, z, c), tp), (place(y, 3 - z, c), tp)
    far_d = (place(3 - y, 3 - z, c), tp)
    other = (place(y, z, 1 - c), tp)
    right, left = (sp, (tp + 1) % 4), (sp, (tp + 3) % 4)
    across = (sp, (tp + 2) % 4)
    ahead, behind = ((sp + 1) % 32, tp), ((sp + 31) % 32, tp)
    chips = [(y, z), (y_in, z), (y, z_in), (y_in, z_in)]
    expert_of = [place(yy, zz, cc) for yy, zz in chips for cc in (c, 1 - c)]

    barrier = pltpu.get_barrier_semaphore()
    partners = [near_y, near_z, far_y, far_z, far_d, other, right, left, across, ahead, behind]
    for partner in partners:
        pl.semaphore_signal(barrier, inc=1, device_id=partner, device_id_type=MESH)

    cp = Copies(send_sem, recv_sem)
    fetches = {}

    def fetch(name, src, dst, i=None):
        i = 9 + len(fetches) if i is None else i
        fetches[name] = pltpu.make_async_copy(src, dst, local_sem.at[i])
        fetches[name].start()

    def strip(k):
        return pl.ds(pl.multiple_of(k * rows, rows), rows)

    conv_v, in_gate_v = buf_gate.at[0, :, :256], buf_gate.at[0, :, 256:]
    out_gate_v = buf_gate.at[1, :, :256]
    fetch("conv", conv_input, conv_v)
    fetch("in_gate", input_gate, in_gate_v)
    fetch("out_gate", output_gate, out_gate_v)
    fetch("taps", taps, taps_v)
    fetch("docs", docs, docs_v)
    fetch("ids", ids, ids_v)
    fetch("route", route_weight, route_v)
    fetch("gain", gain, gain_v)
    fetch("proj0", proj.at[:512], buf_down.at[0])
    fetch("proj1", proj.at[512:], buf_down.at[1])
    fetch("res0", residual.at[:256], rows_x.at[0])
    fetch("res1", residual.at[256:], rows_x.at[1])
    pl.semaphore_wait(barrier, len(partners))

    cp.start("halo_c", conv_input.at[length - 16 :], halo_c, ahead)
    cp.start("halo_g", input_gate.at[length - 16 :], halo_g, ahead)
    cp.start("halo_d", docs.at[8:], halo_d, ahead)
    mine = strip(tp)
    near = (("y", near_y, 1), ("z", near_z, 3))
    for name, dev, slot in near:
        cp.start("gate_" + name, w_gate.at[mine], all_gate.at[slot, mine], dev)
    for name, dev, slot in near:
        cp.start("up_" + name, w_up.at[mine], all_up.at[slot, mine], dev)
    late = pl.ds(pl.multiple_of(((tp + 2) % 4) * rows + rows - DIRECT, DIRECT), DIRECT)
    cp.start("gate_d_y", w_gate.at[late], all_gate.at[1, late], near_y)
    cp.start("up_d_z", w_up.at[late], all_up.at[3, late], near_z)
    for name, dev, slot in near:
        cp.start("down_" + name, w_down, all_down.at[slot], dev)
    cp.start("own_gate", w_gate, all_gate.at[0], other)
    cp.start("own_up", w_up, all_up.at[0], other)
    cp.start("own_down", w_down, all_down.at[0], other)

    for name in ("conv", "in_gate", "out_gate", "taps", "docs"):
        fetches[name].wait()
    for r in range(length // 128):
        doc_rows[8 + r * 128 : 136 + r * 128, :] = jnp.broadcast_to(
            docs_v[r : r + 1, :].astype(F32), (128, 128)
        ).T
    for r in range(0, length, 256):
        product[8 + r : 264 + r, :] = buf_gate[0, r : r + 256, :256].astype(F32) * buf_gate[
            0, r : r + 256, 256:
        ].astype(F32)
    tap = [taps_v[k : k + 1, :].astype(F32) for k in range(3)]

    def convolve(r):
        here = doc_rows[8 + r : 264 + r, :]
        same = [doc_rows[6 + k + r : 262 + k + r, :] == here for k in range(2)]
        for h in (0, 128):
            total = tap[2][:, h : h + 128] * product[8 + r : 264 + r, h : h + 128]
            for k in range(2):
                term = tap[k][:, h : h + 128] * product[6 + k + r : 262 + k + r, h : h + 128]
                total = total + jnp.where(same[k], term, 0.0)
            gated[r : r + 256, h : h + 128] = (
                buf_gate[1, r : r + 256, h : h + 128].astype(F32) * total
            ).astype(BF16)

    for r in range(256, length, 256):
        convolve(r)
    cp.arrived("halo_c")
    cp.arrived("halo_g")
    cp.arrived("halo_d")
    product[:8, :] = (halo_c[...].astype(F32) * halo_g[...].astype(F32))[8:]
    halo_docs = jnp.broadcast_to(halo_d[7:8, :].astype(F32), (128, 128)).T
    doc_rows[:8, :] = jnp.where(sp == 0, -1.0, halo_docs[120:])
    convolve(0)

    for name, dev in (("r", right), ("l", left), ("a", across)):
        cp.start("mix_" + name, gated.at[strip(dev[1])], a2a.at[tp], dev)
    fetch("mix", gated.at[strip(tp)], a2a.at[tp])

    def share(kind, name, part, at):
        store = all_gate if kind == "gate" else all_up
        slot = 1 if name == "y" else 3
        cp.start(f"{kind}_o{part}_{name}", store.at[slot, at], store.at[slot + 1, at], other)

    def turn(kind, way, name, part, at):
        store = all_gate if kind == "gate" else all_up
        slot = 1 if name == "y" else 3
        cp.start(
            f"{kind}_{part}_{name}", store.at[slot, at], store.at[slot, at], right if way == "r" else left
        )

    before, after, opposite = strip((tp + 3) % 4), strip((tp + 1) % 4), strip((tp + 2) % 4)

    def early(k):
        return pl.ds(pl.multiple_of((k % 4) * rows, rows), rows - DIRECT)

    for name in ("y", "z"):
        cp.arrived("gate_" + name)
        turn("gate", "r", name, "r", mine)
        turn("gate", "l", name, "l", mine)
        share("gate", name, "m", mine)

    fetches["ids"].wait()
    fetches["route"].wait()
    experts = lax.broadcasted_iota(jnp.int32, (EXPERTS, rows), 0)
    hit = [ids_v[j : j + 1, :] == experts for j in range(2)]
    used = jnp.where(hit[0], 1.0, jnp.where(hit[1], 1.0, 0.0))
    earlier = lax.broadcasted_iota(jnp.int32, (rows, rows), 0) < lax.broadcasted_iota(jnp.int32, (rows, rows), 1)
    dispatch[...] = jnp.where(earlier, 1.0, 0.0).astype(BF16)
    rank = jnp.dot(used.astype(BF16), dispatch[...], preferred_element_type=F32)
    tables[0, :EXPERTS, :] = jnp.where(used > 0.0, rank, -1.0)
    tables[0, EXPERTS:, :] = jnp.where(hit[0], route_v[0:1, :], jnp.where(hit[1], route_v[1:2, :], 0.0))

    for name, dev, slot in (("y", far_y, 1), ("z", far_z, 2), ("d", far_d, 3)):
        cp.start("table_" + name, tables.at[0], tables.at[slot], dev)

    for name in ("mix", "proj0", "proj1", "res0", "res1", "gain"):
        fetches[name].wait()
    for name in ("r", "l", "a"):
        cp.arrived("mix_" + name)
    step = 512

    def project():
        squares = jnp.zeros((rows, 1), F32)
        for n in range(0, width, step):
            part = jnp.concatenate([rows_x[0, :, n : n + step], rows_x[1, :, n : n + step]], axis=0).astype(F32)
            for j in range(4):
                part = part + jnp.dot(
                    a2a[j],
                    buf_down[j // 2, (j % 2) * 256 : (j % 2 + 1) * 256, n : n + step],
                    preferred_element_type=F32,
                )
            hidden[:, n : n + step] = part
            squares = squares + jnp.sum(part * part, axis=1, keepdims=True)
        scale = lax.rsqrt(squares * (1.0 / width) + epsilon)
        for n in range(0, width, step):
            tok[0, :, n : n + step] = (hidden[:, n : n + step] * scale * gain_v[:, n : n + step]).astype(BF16)

    project()
    cp.start("tok_y", tok.at[0], tok.at[1], far_y)
    cp.start("tok_z", tok.at[0], tok.at[2], far_z)

    def matches(source, pair):
        slot = lax.broadcasted_iota(jnp.int32, (CAP, rows), 0).astype(F32)
        halves, weights = [], []
        for k in range(2):
            e = expert_of[2 * pair + k]
            same = tables[source, pl.ds(e, 1), :] == slot
            halves.append(jnp.where(same, 1.0, 0.0))
            weights.append(jnp.where(same, tables[source, pl.ds(EXPERTS + e, 1), :], 0.0))
        return jnp.concatenate(halves, axis=0), jnp.concatenate(weights, axis=0)

    source_of = [1, 2, 0, 3]

    def gather(i):
        source = source_of[i]
        for pair in range(4):
            dispatch[pair * 128 : (pair + 1) * 128, :] = matches(source, pair)[0].astype(BF16)
        for n in range(0, width, step):
            got = jnp.dot(dispatch[...], tok[source, :, n : n + step], preferred_element_type=F32).astype(BF16)
            for e in range(6):
                rows_x[e, i * CAP : (i + 1) * CAP, n : n + step] = got[e * CAP : (e + 1) * CAP]
            rows_di[i, :, n : n + step] = got[6 * CAP :]

    def weigh(i):
        for pair in range(4):
            combine[:, pair * 128 : (pair + 1) * 128] = matches(source_of[i], pair)[1].T.astype(BF16)

    def scatter(i, cols, store):
        for n in range(cols.start, cols.stop, step):
            total = jnp.dot(combine[:, :384], outs[i, :, n : n + step], preferred_element_type=F32)
            total = total + jnp.dot(combine[:, 384:], returned[i, :, n : n + step], preferred_element_type=F32)
            store(n, total)

    def load(e, slot):
        gate_from = w_gate if e == 0 else all_gate.at[e - 1]
        up_from = w_up if e == 0 else all_up.at[e - 1]
        down_from = w_down if e == 0 else all_down.at[e - 1]
        fetch(f"g{slot}", gate_from, buf_gate.at[slot], slot * 3)
        fetch(f"u{slot}", up_from, buf_up.at[slot], slot * 3 + 1)
        fetch(f"d{slot}", down_from, buf_down.at[slot], slot * 3 + 2)

    def loaded(slot):
        for kind in "gud":
            fetches[f"{kind}{slot}"].wait()

    def activate(slot, left_ref, high):
        for n in range(0, 512, 256):
            left_side = left_ref[...]
            gate_val = jnp.dot(left_side, buf_gate[slot, :, n : n + 256], preferred_element_type=F32)
            up_val = jnp.dot(left_side, buf_up[slot, :, n : n + 256], preferred_element_type=F32)
            act[:high, n : n + 256] = (gate_val / (1.0 + jnp.exp(-gate_val)) * up_val).astype(BF16)

    def local(e, slot, batch):
        activate(slot, rows_x.at[e, batch * 128 : (batch + 1) * 128], 128)
        for n in range(0, width, step):
            got = jnp.dot(act[...], buf_down[slot, :, n : n + step], preferred_element_type=F32).astype(BF16)
            for k in range(2):
                outs[2 * batch + k, e * CAP : (e + 1) * CAP, n : n + step] = got[k * CAP : (k + 1) * CAP]

    def distant(e, slot, i):
        at = slice((e % 2) * CAP, (e % 2 + 1) * CAP)
        activate(slot, rows_in.at[i, at], CAP)
        for n in range(0, width, step):
            outs_far[i, at, n : n + step] = jnp.dot(
                act[:CAP, :], buf_down[slot, :, n : n + step], preferred_element_type=F32
            ).astype(BF16)

    def ask(i):
        for k in range(2):
            at = slice(k * CAP, (k + 1) * CAP)
            by_y = k == 1 if i == 3 else i != 1
            cp.start(f"ask{i}{k}", rows_di.at[i, at], rows_in.at[i, at], near_y if by_y else near_z)

    def answer(e, i, order):
        at = slice((e % 2) * CAP, (e % 2 + 1) * CAP)
        for half in order:
            cols = A_COLS if half == "a" else B_COLS
            cp.start(
                f"ans{i}{e % 2}{half}",
                outs_far.at[i, at, cols],
                returned.at[i, at, cols],
                near_z if e < 4 else near_y,
            )

    def answered(i, half):
        for k in range(2):
            cp.arrived(f"ans{i}{k}{half}")

    gather(2)
    cp.arrived("up_y")
    turn("up", "r", "y", "r", mine)
    turn("up", "l", "y", "l", mine)
    share("up", "y", "m", mine)
    cp.arrived("gate_r_y")
    turn("gate", "r", "y", "f", early(tp + 3))
    share("gate", "y", "r", before)
    cp.arrived("up_z")
    turn("up", "r", "z", "r", mine)
    share("up", "z", "m", mine)
    cp.arrived("gate_l_y")
    share("gate", "y", "l", after)
    cp.arrived("gate_r_z")
    turn("gate", "r", "z", "f", before)
    share("gate", "z", "r", before)
    cp.arrived("up_d_z")
    share("up", "z", "d", late)
    cp.arrived("gate_l_z")
    share("gate", "z", "l", after)
    cp.arrived("up_l_y")
    turn("up", "l", "y", "f", after)
    turn("up", "l", "z", "l", mine)
    share("up", "y", "l", after)
    cp.arrived("up_r_y")
    share("up", "y", "r", before)
    for name in ("gate", "up", "down"):
        cp.arrived("own_" + name)
    load(0, 0)
    load(1, 1)
    cp.arrived("gate_f_y")
    share("gate", "y", "f", early(tp + 2))
    cp.arrived("gate_d_y")
    share("gate", "y", "d", late)
    cp.arrived("up_f_y")
    share("up", "y", "f", opposite)

    cp.arrived("tok_y")
    cp.start("tok_fy", tok.at[1, :HALF], tok.at[3, :HALF], far_z)
    cp.arrived("tok_z")
    cp.start("tok_fz", tok.at[2, HALF:], tok.at[3, HALF:], far_y)
    cp.arrived("table_y")
    gather(0)
    ask(0)
    cp.arrived("table_z")
    gather(1)
    ask(1)

    cp.arrived("down_y")
    cp.start("down_o_y", all_down.at[1], all_down.at[2], other)
    load(2, 2)
    cp.arrived("up_l_z")
    turn("up", "l", "z", "f", early(tp + 1))
    share("up", "z", "l", after)
    loaded(0)
    local(0, 0, 0)
    for kind, parts in (("gate", "mrlfd"), ("up", "mrlf")):
        for part in parts:
            cp.arrived(f"{kind}_o{part}_y")
    loaded(1)
    local(1, 1, 0)
    cp.arrived("up_r_z")
    share("up", "z", "r", before)
    cp.arrived("down_z")
    cp.start("down_o_z", all_down.at[3], all_down.at[4], other)
    loaded(2)
    local(2, 2, 0)
    cp.arrived("down_o_y")
    load(3, 0)
    cp.arrived("gate_f_z")
    share("gate", "z", "f", opposite)
    cp.arrived("up_f_z")
    share("up", "z", "f", early(tp + 2))
    load(4, 1)
    cp.arrived("ask10")
    distant(2, 2, 1)
    answer(2, 1, "b")
    loaded(0)
    local(3, 0, 0)
    cp.arrived("ask11")
    distant(3, 0, 1)
    answer(3, 1, "b")
    for kind, parts in (("gate", "mrlf"), ("up", "mrlfd")):
        for part in parts:
            cp.arrived(f"{kind}_o{part}_z")
    cp.arrived("down_o_z")
    load(5, 2)
    load(2, 0)
    cp.arrived("ask00")
    loaded(1)
    distant(4, 1, 0)
    answer(4, 0, "a")
    local(4, 1, 0)
    cp.arrived("ask01")
    loaded(2)
    distant(5, 2, 0)
    answer(5, 0, "a")
    local(5, 2, 0)

    def into(k, name=None, to=None, dev=None):
        def store(n, total):
            tok[k, :, n : n + step] = total.astype(BF16)
            if name is not None:
                r = n // step % 2
                cp.start(f"{name}{r}", tok.at[k, :, n : n + step], land.at[to, :, r * step : (r + 1) * step], dev)

        return store

    cp.sent("tok_fz")
    weigh(1)
    answered(1, "b")
    scatter(1, B_COLS, into(2, "pure_z", 1, far_z))
    cp.arrived("tok_fy")
    cp.arrived("tok_fz")
    cp.arrived("table_d")
    gather(3)
    ask(3)
    answer(4, 0, "b")
    answer(5, 0, "b")
    cp.sent("tok_fy")
    weigh(0)
    answered(0, "a")
    scatter(0, A_COLS, into(1, "pure_y", 0, far_y))

    local(5, 2, 1)
    local(4, 1, 1)
    loaded(0)
    local(2, 0, 1)
    cp.arrived("ask30")
    distant(2, 0, 3)
    answer(2, 3, "ba")
    load(3, 0)
    cp.arrived("ask31")
    distant(5, 2, 3)
    answer(5, 3, "ba")
    load(0, 2)
    answer(2, 1, "a")
    answer(3, 1, "a")
    ask(2)
    answered(0, "b")
    scatter(0, B_COLS, into(1))
    loaded(0)
    local(3, 0, 1)
    load(1, 0)
    loaded(2)
    local(0, 2, 1)
    load(5, 2)
    weigh(3)
    loaded(0)
    local(1, 0, 1)
    answered(3, "b")
    scatter(3, B_COLS, into(3, "diag_z", 3, far_z))
    answered(3, "a")
    scatter(3, A_COLS, into(3, "diag_y", 2, far_y))
    weigh(1)
    answered(1, "a")
    scatter(1, A_COLS, into(2))
    cp.arrived("ask20")
    distant(4, 1, 2)
    answer(4, 2, "ab")
    cp.arrived("ask21")
    loaded(2)
    distant(5, 2, 2)
    answer(5, 2, "ab")

    def onto_hidden(n, total):
        hidden[:, n : n + step] = hidden[:, n : n + step] + total

    weigh(2)
    answered(2, "a")
    answered(2, "b")
    scatter(2, A_COLS, onto_hidden)
    scatter(2, B_COLS, onto_hidden)
    for r in range(2):
        cp.arrived(f"pure_z{r}")
        cp.arrived(f"pure_y{r}")
    hidden[:, A_COLS] = hidden[:, A_COLS] + land[0].astype(F32)
    hidden[:, B_COLS] = hidden[:, B_COLS] + land[1].astype(F32)
    fetch("hidden", hidden, hidden_out)

    for r in range(2):
        at, to_a, to_b = (slice(k + r * step, k + (r + 1) * step) for k in (0, 0, 1024))
        cp.arrived(f"diag_z{r}")
        tok[1, :, to_b] = (tok[1, :, to_b].astype(F32) + land[3, :, at].astype(F32)).astype(BF16)
        cp.start(f"fwd_y{r}", tok.at[1, :, to_b], far_out.at[:, to_b], far_y)
        cp.arrived(f"diag_y{r}")
        tok[2, :, to_a] = (tok[2, :, to_a].astype(F32) + land[2, :, at].astype(F32)).astype(BF16)
        cp.start(f"fwd_z{r}", tok.at[2, :, to_a], far_out.at[:, to_a], far_z)
    fetches["hidden"].wait()
    for name in [name for name in cp.unsent if not name.startswith("fwd")]:
        cp.sent(name)
    for r in range(2):
        cp.arrived(f"fwd_z{r}")
        cp.arrived(f"fwd_y{r}")
    cp.finish()


def layer(*operands):
    residual, w_gate = operands[0], operands[10]
    rows, width = residual.shape
    hid = w_gate.shape[1]
    length, channels = operands[1].shape
    any_spec = pl.BlockSpec(memory_space=pl.ANY)
    shapes = (
        jax.ShapeDtypeStruct((rows, width), F32),
        jax.ShapeDtypeStruct((rows, width), BF16),
        jax.ShapeDtypeStruct((5, width, hid), BF16),
        jax.ShapeDtypeStruct((5, width, hid), BF16),
        jax.ShapeDtypeStruct((5, hid, width), BF16),
    )
    hidden, far = pl.pallas_call(
        layer_kernel,
        out_shape=shapes,
        in_specs=[any_spec] * len(operands),
        out_specs=(any_spec,) * 5,
        scratch_shapes=[
            pltpu.VMEM((3, channels), BF16),
            pltpu.VMEM((length // 128, 128), jnp.int32),
            pltpu.VMEM((2, rows), jnp.int32),
            pltpu.VMEM((2, rows), F32),
            pltpu.VMEM((16, channels), BF16),
            pltpu.VMEM((16, channels), BF16),
            pltpu.VMEM((8, 128), jnp.int32),
            pltpu.VMEM((length + 8, channels), F32),
            pltpu.VMEM((length + 8, 128), F32),
            pltpu.VMEM((length, channels), BF16),
            pltpu.VMEM((4, rows, channels), BF16),
            pltpu.VMEM((1, width), F32),
            pltpu.VMEM((rows, width), F32),
            pltpu.VMEM((4, rows, width), BF16),
            pltpu.VMEM((4, 2 * EXPERTS, rows), F32),
            pltpu.VMEM((512, rows), BF16),
            pltpu.VMEM((rows, 512), BF16),
            pltpu.VMEM((6, 256, width), BF16),
            pltpu.VMEM((4, 128, width), BF16),
            pltpu.VMEM((4, 128, width), BF16),
            pltpu.VMEM((128, hid), BF16),
            pltpu.VMEM((4, 384, width), BF16),
            pltpu.VMEM((4, 128, width), BF16),
            pltpu.VMEM((4, 128, width), BF16),
            pltpu.VMEM((4, rows, width // 2), BF16),
            pltpu.VMEM((3, width, hid), BF16),
            pltpu.VMEM((3, width, hid), BF16),
            pltpu.VMEM((3, hid, width), BF16),
            pltpu.SemaphoreType.DMA((COPIES,)),
            pltpu.SemaphoreType.DMA((COPIES,)),
            pltpu.SemaphoreType.DMA((LOCALS + 16,)),
        ],
        compiler_params=pltpu.CompilerParams(
            collective_id=0, has_side_effects=True, vmem_limit_bytes=67043328
        ),
        name="layer",
    )(*operands)[:2]
    return (hidden + far.astype(F32)).astype(BF16)


def per_device(
    residual_in,
    conv_input,
    input_gate,
    output_gate,
    conv_taps,
    doc_ids,
    proj_weight,
    norm_gain,
    expert_ids,
    expert_weight,
    w_gate,
    w_up,
    w_down,
):
    return layer(
        residual_in,
        conv_input,
        input_gate,
        output_gate,
        conv_taps,
        doc_ids.reshape(-1, 128),
        proj_weight,
        norm_gain[None, :],
        expert_ids.T,
        expert_weight.T,
        w_gate[0],
        w_up[0],
        w_down[0],
    )


def solution(mesh):
    return jax.shard_map(
        per_device,
        mesh=mesh,
        in_specs=(
            P(("sp", "tp"), None),
            P("sp", "tp"),
            P("sp", "tp"),
            P("sp", "tp"),
            P(None, "tp"),
            P("sp"),
            P(),
            P(),
            P(("sp", "tp"), None),
            P(("sp", "tp"), None),
            P("sp", None, None),
            P("sp", None, None),
            P("sp", None, None),
        ),
        out_specs=P(("sp", "tp"), None),
        check_vma=False,
    )
```
